256 devices in a mesh: sp: 32 (over z, y), tp: 8 (over x, core).
Axes of the slice: x: 4, y: 4, z: 8, core: 2. Of those that a mesh axis runs over, the one named last changes fastest.
Arguments:
- tokens: bfloat16 [16384, 2048], P('sp', 'tp'), may hold values from -64 to 64
- conv_input: bfloat16 [2048, 1024], P(None, 'tp'), may hold values from -0.125 to 0.125
- conv_inner: bfloat16 [2048, 1024], P(None, 'tp'), may hold values from -0.125 to 0.125
- conv_outer: bfloat16 [2048, 1024], P(None, 'tp'), may hold values from -0.125 to 0.125
- conv_gate: bfloat16 [2048, 1024], P(None, 'tp'), may hold values from -0.125 to 0.125
- conv_taps: bfloat16 [3, 1024], P(None, 'tp'), may hold values from -3.5 to 3.5
- query_proj: bfloat16 [2048, 1536], P(None, 'tp'), may hold values from -8 to 8
- latent_proj: bfloat16 [2048, 256], replicated, may hold values from -1 to 1
- rope_proj: bfloat16 [2048, 32], replicated, may hold values from -0.125 to 0.125
- latent_gain: float32 [256], replicated, may hold values from 0.1 to 1.9
- key_up: bfloat16 [256, 1024], P(None, 'tp'), may hold values from -2 to 2
- value_up: bfloat16 [256, 1024], P(None, 'tp'), may hold values from -0.375 to 0.375
- attn_gate: bfloat16 [2048, 1024], P(None, 'tp'), may hold values from -0.125 to 0.125
- conv_down: bfloat16 [1024, 2048], P('tp'), may hold values from -0.1875 to 0.1875
- attn_down: bfloat16 [1024, 2048], P('tp'), may hold values from -0.75 to 0.75
Outputs:
- layer_out: bfloat16 [16384, 2048], P(('sp', 'tp'))
The draws below stay inside these ranges and needn't reach their ends.
All inputs are finite; a program needn't handle non-finite values.
Results may differ from the reference program's by a relative error of at most 0.014.
Values may be sent and summed in bfloat16 or wider, within the bound.
A program may use at most 128 MiB of HBM per device.

```python
import math
import jax
import jax.numpy as jnp
from jax import lax

D = 2048
D_CONV = 1024
HEADS = 16
NOPE = 64
ROPE = 32
VDIM = 64
KV = 256
GRID_W = 64
SEQ = 16384
N_TP = 8


def weight_pair(key):
    down_part = jnp.clip(jax.random.normal(jax.random.fold_in(key, 101), (D, KV), jnp.float32), -6.0, 6.0) * D ** (-0.5)
    up_part = jnp.clip(jax.random.normal(jax.random.fold_in(key, 102), (KV, HEADS * NOPE), jnp.float32), -6.0, 6.0) * KV ** (-0.5)
    return (down_part, up_part)


def draw_latent_proj(key, part):
    return jnp.clip(weight_pair(key)[0], -1.0, 1.0).astype(jnp.bfloat16)


def draw_key_up(key, part):
    return jnp.clip(weight_pair(key)[1], -2.0, 2.0).astype(jnp.bfloat16)


def draw_tokens(key, part):
    column = jnp.arange(D, dtype=jnp.float32) / max(D - 1, 1)
    col_noise = jax.random.uniform(jax.random.fold_in(key, 201), (D,), jnp.float32)
    row_exp = jax.random.uniform(jax.random.fold_in(key, 202), (SEQ,), jnp.float32, -0.5, 0.5)
    base_draw = jnp.clip(jax.random.normal(jax.random.fold_in(key, 204), (SEQ, D), jnp.float32), -6.0, 6.0)
    col_exp = 0.5 * column + 0.5 * col_noise - 0.5
    scaling = (10.0 ** row_exp)[:, None] * (10.0 ** col_exp)[None, :]
    values = base_draw * scaling
    return jnp.clip(values, -64.0, 64.0).astype(jnp.bfloat16)


def draw_query_proj(key, part):
    spread = (6.0 / D) ** 0.5
    whole_draw = jnp.clip(jax.random.normal(jax.random.fold_in(key, 303), (D, HEADS, NOPE + ROPE), jnp.float32), -6.0, 6.0) * spread
    return jnp.clip(whole_draw, -8.0, 8.0).reshape(D, HEADS * (NOPE + ROPE)).astype(jnp.bfloat16)


def block_levels(rng, shape, cuts, low, high):
    gain = 1.0
    for axis_at, shards_of in cuts:
        draws = jax.random.uniform(jax.random.fold_in(jax.random.fold_in(rng, 6), axis_at), (shards_of,), jnp.float32, low / len(cuts), high / len(cuts))
        gain = gain * jnp.repeat(jnp.exp(draws), shape[axis_at] // shards_of).reshape((-1,) + (1,) * (len(shape) - 1 - axis_at))
    return gain


def bell_draw(key, shape, width, bound, split=(), kind=jnp.bfloat16):
    array = width * jax.random.normal(key, shape, jnp.float32)
    if split:
        array = array * block_levels(key, shape, split, -0.22, 0.18)
    return jnp.clip(array, -bound, bound).astype(kind)


def setup_inputs(seed: int = 0) -> dict:
    splits = jax.random.split(jax.random.key(seed), 16)
    return {
        "tokens": draw_tokens(jax.random.fold_in(splits[15], 71), 0),
        "conv_input": bell_draw(splits[1], (D, D_CONV), D ** -0.5, 0.125, ((1, 8),)),
        "conv_inner": bell_draw(splits[2], (D, D_CONV), D ** -0.5, 0.125, ((1, 8),)),
        "conv_outer": bell_draw(splits[3], (D, D_CONV), D ** -0.5, 0.125, ((1, 8),)),
        "conv_gate": bell_draw(splits[4], (D, D_CONV), D ** -0.5, 0.125, ((1, 8),)),
        "conv_taps": bell_draw(splits[5], (3, D_CONV), 3 ** -0.5, 3.5, ((1, 8),)),
        "query_proj": draw_query_proj(jax.random.fold_in(splits[15], 71), 0),
        "latent_proj": draw_latent_proj(jax.random.fold_in(splits[15], 71), 0),
        "rope_proj": bell_draw(splits[8], (D, ROPE), D ** -0.5, 0.125),
        "latent_gain": jnp.clip(1.0 + 0.18 * jax.random.normal(splits[9], (KV,), jnp.float32), 0.1, 1.9),
        "key_up": draw_key_up(jax.random.fold_in(splits[15], 71), 0),
        "value_up": bell_draw(splits[11], (KV, HEADS * VDIM), KV ** -0.5, 0.375, ((1, 8),)),
        "attn_gate": bell_draw(splits[12], (D, HEADS * VDIM), D ** -0.5, 0.125, ((1, 8),)),
        "conv_down": bell_draw(splits[13], (D_CONV, D), D_CONV ** -0.5, 0.1875, ((0, 8),)),
        "attn_down": bell_draw(splits[14], (HEADS * VDIM, D), (HEADS * VDIM // 16) ** -0.5, 0.75, ((0, 8),)),
    }


rms_eps = 1e-06
rope_theta = 10000.0

def rounded(values):
    return lax.optimization_barrier(values.astype(jnp.bfloat16))

def axial_tables(positions, rope_width, grid_width):
    quarter = rope_width // 4
    frequency = rope_theta ** (-jnp.arange(quarter, dtype=jnp.float32) * 2.0 / (rope_width // 2))
    grid_row = (positions // grid_width).astype(jnp.float32)
    grid_col = (positions % grid_width).astype(jnp.float32)
    row_angle = grid_row[:, None] * frequency[None, :]
    col_angle = grid_col[:, None] * frequency[None, :]
    return (jnp.cos(row_angle), jnp.sin(row_angle), jnp.cos(col_angle), jnp.sin(col_angle))

def turn_half(vector, cos_table, sin_table):
    half_width = vector.shape[-1] // 2
    leading = vector[..., :half_width]
    trailing = vector[..., half_width:]
    return jnp.concatenate([leading * cos_table - trailing * sin_table, trailing * cos_table + leading * sin_table], axis=-1)

def axial_turn(vector, tables):
    half_width = vector.shape[-1] // 2
    return jnp.concatenate([turn_half(vector[..., :half_width], tables[0], tables[1]), turn_half(vector[..., half_width:], tables[2], tables[3])], axis=-1)

def reference(tokens, conv_input, conv_inner, conv_outer, conv_gate, conv_taps, query_proj, latent_proj, rope_proj, latent_gain, key_up, value_up, attn_gate, conv_down, attn_down):
    seq_len = tokens.shape[0]
    widened = tokens.astype(jnp.float32)
    row_scale = lax.rsqrt(lax.optimization_barrier(jnp.mean(widened * widened, axis=1, keepdims=True)) + rms_eps)

    def project(matrix):
        return jnp.dot(tokens, matrix, preferred_element_type=jnp.float32) * row_scale
    value_in = rounded(project(conv_input)).astype(jnp.float32)
    inner_in = rounded(project(conv_inner)).astype(jnp.float32)
    outer_in = rounded(project(conv_outer)).astype(jnp.float32)
    gate_in = rounded(project(conv_gate)).astype(jnp.float32)
    conv_product = rounded(inner_in * value_in).astype(jnp.float32)
    padded = jnp.pad(conv_product, ((1, 1), (0, 0)))
    tap_weights = conv_taps.astype(jnp.float32)
    conv_mixed = padded[:-2] * tap_weights[0] + padded[1:-1] * tap_weights[1] + padded[2:] * tap_weights[2]
    conv_out = (jax.nn.silu(gate_in) * outer_in * conv_mixed).astype(jnp.bfloat16)
    positions = jnp.arange(seq_len, dtype=jnp.int32)
    tables = axial_tables(positions, ROPE, GRID_W)
    head_tables = tuple((grid_table[:, None, :] for grid_table in tables))
    queries = project(query_proj).reshape(seq_len, HEADS, NOPE + ROPE)
    query_nope = queries[..., :NOPE].astype(jnp.bfloat16)
    query_rope = axial_turn(queries[..., NOPE:], head_tables).astype(jnp.bfloat16)
    latent = project(latent_proj)
    latent = (latent * lax.rsqrt(lax.optimization_barrier(jnp.mean(latent * latent, axis=1, keepdims=True)) + rms_eps) * latent_gain).astype(jnp.bfloat16)
    key_rope = axial_turn(project(rope_proj), tables).astype(jnp.bfloat16)
    key_nope = jnp.dot(latent, key_up, preferred_element_type=jnp.float32).astype(jnp.bfloat16).reshape(seq_len, HEADS, NOPE)
    key_values = jnp.dot(latent, value_up, preferred_element_type=jnp.float32).astype(jnp.bfloat16).reshape(seq_len, HEADS, VDIM)
    gate_attn = rounded(project(attn_gate)).astype(jnp.float32)
    key_wide = key_nope.astype(jnp.float32)
    rope_wide = key_rope.astype(jnp.float32)
    value_wide = key_values.astype(jnp.float32)
    block_rows = math.gcd(seq_len, 256)
    score_scale = (NOPE + ROPE) ** (-0.5)

    def attend_block(block_pair):
        nope_block, rope_block = block_pair
        scores = jnp.einsum('qhd,khd->hqk', nope_block.astype(jnp.float32), key_wide)
        scores = (scores + jnp.einsum('qhd,kd->hqk', rope_block.astype(jnp.float32), rope_wide)) * score_scale
        row_top = lax.optimization_barrier(jnp.max(scores, axis=2, keepdims=True))
        weights = jnp.exp(scores - row_top)
        weight_total = lax.optimization_barrier(jnp.sum(weights, axis=2))
        narrow = rounded(weights).astype(jnp.float32)
        attended = jnp.einsum('hqk,khd->qhd', narrow, value_wide) / weight_total.T[:, :, None]
        return attended.reshape(attended.shape[0], HEADS * VDIM)
    attended = lax.map(attend_block, (query_nope.reshape(-1, block_rows, HEADS, NOPE), query_rope.reshape(-1, block_rows, HEADS, ROPE)))
    attended = attended.reshape(seq_len, HEADS * VDIM)
    attn_out = (jax.nn.silu(gate_attn) * attended).astype(jnp.bfloat16)
    conv_width = D_CONV // N_TP
    head_width = HEADS // N_TP * VDIM
    conv_groups = conv_out.reshape(seq_len, N_TP, conv_width).transpose(1, 0, 2)
    attn_groups = attn_out.reshape(seq_len, N_TP, head_width).transpose(1, 0, 2)
    conv_blocks = conv_down.reshape(N_TP, conv_width, conv_down.shape[1])
    attn_blocks = attn_down.reshape(N_TP, head_width, attn_down.shape[1])

    def add_group(running_sum, group_terms):
        conv_part, conv_matrix, attn_part, attn_matrix = group_terms
        partial_sum = jnp.dot(conv_part, conv_matrix, preferred_element_type=jnp.float32) + jnp.dot(attn_part, attn_matrix, preferred_element_type=jnp.float32)
        return (running_sum + rounded(partial_sum).astype(jnp.float32), None)
    zeroed = jnp.zeros((seq_len, conv_down.shape[1]), jnp.float32)
    summed = lax.scan(add_group, zeroed, (conv_groups, conv_blocks, attn_groups, attn_blocks))[0]
    return summed.astype(jnp.bfloat16)
```

```python
import math

import jax
import jax.numpy as jnp
from jax import lax
from jax.experimental import pallas as pl
from jax.experimental.pallas import tpu as pltpu
from jax.sharding import PartitionSpec as P

NOPE, ROPE, VDIM, GRID_W = 64, 32, 64, 64
EPS = 1e-06
THETA = 10000.0
D = 2048
T = 512
FB = 256
NX, NY, NZ = 4, 4, 8
KEYS = NZ * T
PIECE = T + 64
HALF = PIECE // 2
SUB = HALF // 2
VROWS = VDIM + 16
CHUNK = 512
N_REMOTE = 80
N_LOCAL = 16
MESH = pl.DeviceIdType.MESH
F32, BF16 = jnp.float32, jnp.bfloat16


def iota(shape, dim):
    return lax.broadcasted_iota(jnp.int32, shape, dim)


def mm(a, b):
    return jnp.dot(a, b, preferred_element_type=F32)


def silu(v):
    return v * (1.0 / (1.0 + jnp.exp(-v)))


def selection(rows, cols, test):
    return jnp.where(test(iota((rows, cols), 0), iota((rows, cols), 1)), 1.0, 0.0).astype(BF16)


def layer_kernel(
    tokens, conv_input, conv_inner, conv_outer, conv_gate, conv_taps, query_proj, latent_proj,
    rope_proj, latent_gain, key_up, value_up, attn_gate, conv_down, attn_down,
    out,
    xall, w5, wq_raw, wq, wl, wr_raw, wr, ku_raw, ku2, vu_raw, wd, taps, gain,
    a5, al, aq, ar, ss, cos_t, sin_t,
    msg, qs, kall, vt, sbuf, acc,
    om, ostat, ro, rstat, relay, relay_stat,
    cprod, halo, conv_out, lhs, p_send, p_recv, own, pair2, pair1, pair3, turn_a, turn_b, from_l, from_r,
    send_sems, recv_sems, local_sems,
):
    sp, tp = lax.axis_index("sp"), lax.axis_index("tp")
    z, y = sp // NY, sp % NY
    x, core = tp // 2, tp % 2
    other = 1 - core
    dev = lambda s, t: {"sp": s, "tp": t}
    partner = dev(sp, x * 2 + other)
    xr, xl = dev(sp, (x + 1) % NX * 2 + core), dev(sp, (x + NX - 1) % NX * 2 + core)
    yr, yl = dev(z * NY + (y + 1) % NY, tp), dev(z * NY + (y + NY - 1) % NY, tp)
    zr, zl = dev((z + 1) % NZ * NY + y, tp), dev((z + NZ - 1) % NZ * NY + y, tp)
    span_next, span_prev = dev((sp + 1) % (NZ * NY), tp), dev((sp + NZ * NY - 1) % (NZ * NY), tp)

    started = []

    def remote(src, dst, to):
        k = len(started)
        copy = pltpu.make_async_remote_copy(
            src_ref=src, dst_ref=dst, send_sem=send_sems.at[k], recv_sem=recv_sems.at[k],
            device_id=to, device_id_type=MESH,
        )
        copy.start()
        started.append(copy)
        return copy

    locals_ = []

    def load(src, dst):
        copy = pltpu.make_async_copy(src, dst, local_sems.at[len(locals_)])
        copy.start()
        locals_.append(copy)
        return copy

    own_block = load(tokens, xall.at[0])
    loads_rope = [load(rope_proj, wr_raw), load(query_proj, wq_raw), load(key_up, ku_raw), load(value_up, vu_raw)]
    loads_proj = [
        load(w, w5.at[:, pl.ds(128 * k, 128)])
        for k, w in enumerate((conv_input, conv_inner, conv_outer, conv_gate, attn_gate))
    ]
    loads_proj.append(load(latent_proj, wl))
    loads_late = [load(conv_taps, taps), load(latent_gain, gain)]
    loads_late += [load(conv_down, wd.at[pl.ds(0, 128), :]), load(attn_down, wd.at[pl.ds(128, 128), :])]

    barrier = pltpu.get_barrier_semaphore()
    peers = (partner, xr, xl, yr, yl, zr, zl, span_next, span_prev)
    for to in peers:
        pl.semaphore_signal(barrier, inc=1, device_id=to, device_id_type=MESH)
    pl.semaphore_wait(barrier, len(peers))

    own_block.wait()
    h0, h1 = pl.ds(0, T // 2), pl.ds(T // 2, T // 2)
    r0 = remote(xall.at[0, h0], xall.at[1, h0], xr)
    l0 = remote(xall.at[0, h1], xall.at[2, h1], xl)
    r1 = remote(xall.at[0, h1], xall.at[1, h1], xr)
    l1 = remote(xall.at[0, h0], xall.at[2, h0], xl)
    d0 = remote(xall.at[0], xall.at[4], partner)

    for c in loads_rope:
        c.wait()
    e_q = selection(192, 256, lambda r, c: (c % 128 < 96) & (r == c // 128 * 96 + c % 128))

    def widen(i, _):
        rows = pl.ds(pl.multiple_of(i * 256, 256), 256)
        wq[rows, :] = mm(wq_raw[rows, :], e_q).astype(BF16)
        wr[rows, :] = mm(wr_raw[rows, :], selection(32, 128, lambda r, c: r == c)).astype(BF16)
        return 0

    lax.fori_loop(0, D // 256, widen, 0)
    ku2[...] = mm(
        ku_raw[...], selection(128, 256, lambda r, c: (c % 128 < 64) & (r == c // 128 * 64 + c % 128))
    ).astype(BF16)
    token = iota((T, 128), 0) + sp * T
    lane = iota((T, 128), 1)
    freq = jnp.zeros((T, 128), F32)
    for j in range(8):
        freq = jnp.where(lane % 8 == j, float(THETA ** (-2.0 * j / 16)), freq)
    grid_at = jnp.where(lane % 32 < 16, token // GRID_W, token % GRID_W).astype(F32)
    angle = grid_at * freq
    cos_t[...] = jnp.cos(angle)
    sin_t[...] = jnp.sin(angle) * jnp.where(lane % 16 < 8, -1.0, 1.0)
    for i in range(NY):
        for h in range(2):
            qs[i, h, pl.ds(96, 32), :] = jnp.zeros((32, T), BF16)
    for h in range(2):
        vt[h, pl.ds(VDIM, 16), :] = jnp.where(iota((16, KEYS), 0) == 0, 1.0, 0.0).astype(BF16)
    for c in loads_proj:
        c.wait()

    def project(slot, chip, c, first=False):
        block = pl.multiple_of((chip * 2 + c) * FB, FB)

        def rows_of(i, _):
            rows = pl.ds(pl.multiple_of(i * 256, 256), 256)
            v = xall[slot, rows, :]
            wide = v.astype(F32)
            squares = wide[:, :128] * wide[:, :128] + wide[:, 128:] * wide[:, 128:]
            for total, w in ((a5, w5), (al, wl), (aq, wq), (ar, wr)):
                term = mm(v, w[pl.ds(block, FB), :])
                total[rows, :] = term if first else total[rows, :] + term
            ss[rows, :] = squares if first else ss[rows, :] + squares
            return 0

        lax.fori_loop(0, T // 256, rows_of, 0)

    left, right, across = (x + NX - 1) % NX, (x + 1) % NX, (x + 2) % NX
    r0.wait_recv()
    r2 = remote(xall.at[1, h0], xall.at[3, h0], xr)
    l0.wait_recv()
    l2 = remote(xall.at[2, h1], xall.at[3, h1], xl)
    project(0, x, core, first=True)
    d0.wait_recv()
    project(4, x, other)
    r1.wait_recv()
    d1 = remote(xall.at[1], xall.at[5], partner)
    l1.wait_recv()
    d2 = remote(xall.at[2], xall.at[6], partner)
    project(1, left, core)
    project(2, right, core)
    d1.wait_recv()
    project(5, left, other)
    d2.wait_recv()
    project(6, right, other)
    r2.wait_recv()
    d3a = remote(xall.at[3, h0], xall.at[7, h0], partner)
    l2.wait_recv()
    d3b = remote(xall.at[3, h1], xall.at[7, h1], partner)
    project(3, across, core)
    d3a.wait_recv()
    d3b.wait_recv()
    project(7, across, other)
    for c in loads_late:
        c.wait()

    scale = lax.rsqrt(jnp.sum(ss[...], axis=1, keepdims=True) / D + EPS)
    zl_ = al[...] * scale
    latent = zl_ * lax.rsqrt(jnp.mean(zl_ * zl_, axis=1, keepdims=True) + EPS) * gain[...].reshape(1, 256)
    latent = latent.astype(BF16)
    msg[0, 0] = latent[:HALF]
    msg[0, 1, pl.ds(0, T - HALF), :] = latent[HALF:]

    def turned(v):
        swapped = jnp.where(lane % 16 < 8, pltpu.roll(v, 120, 1), pltpu.roll(v, 8, 1))
        return v * cos_t[...] + swapped * sin_t[...]

    key_rope = turned(ar[...] * scale).astype(BF16)
    packed = jnp.zeros((128, 128), F32)
    for g in range(4):
        place = selection(128, 128, lambda r, c, g=g: (r < 32) & (c == r + 32 * g))
        packed = packed + mm(key_rope[128 * g : 128 * (g + 1)], place)
    packed = packed.astype(BF16)
    msg[0, 1, pl.ds(T - HALF, 64), pl.ds(0, 128)] = packed[:64]
    msg[0, 1, pl.ds(T - HALF, 64), pl.ds(128, 128)] = packed[64:]

    s0, s1 = pl.ds(0, SUB), pl.ds(SUB, SUB)

    def key_send(step, sub, to_right):
        d_from, d_to = (step, step + 1) if to_right else ((NZ - step) % NZ, NZ - 1 - step)
        return remote(msg.at[d_from, core, sub], msg.at[d_to, core, sub], zr if to_right else zl)

    zr_a, zl_b = key_send(0, s0, True), key_send(0, s1, False)
    zr_b, zl_a = key_send(0, s1, True), key_send(0, s0, False)

    q_scale = scale * ((NOPE + ROPE) ** (-0.5) * math.log2(math.e))
    for h in range(2):
        v = aq[:, 128 * h : 128 * (h + 1)] * q_scale
        v = jnp.where((lane >= 64) & (lane < 96), turned(v), v)
        qs[0, h, pl.ds(0, 96), :] = jnp.transpose(v)[:96].astype(BF16)
    q96 = pl.ds(0, 96)
    qr0 = remote(qs.at[0, 0, q96], qs.at[1, 0, q96], yr)
    ql0 = remote(qs.at[0, 1, q96], qs.at[2, 1, q96], yl)
    qr1 = remote(qs.at[0, 1, q96], qs.at[1, 1, q96], yr)
    ql1 = remote(qs.at[0, 0, q96], qs.at[2, 0, q96], yl)

    rounded = lambda k: (a5[:, 128 * k : 128 * (k + 1)] * scale).astype(BF16).astype(F32)
    cprod[...] = (rounded(1) * rounded(0)).astype(BF16)
    to_next = remote(cprod.at[pl.ds(T - 16, 16)], halo.at[0], span_next)
    to_prev = remote(cprod.at[pl.ds(0, 16)], halo.at[1], span_prev)

    vu_t = jnp.transpose(vu_raw[...].astype(F32)).astype(BF16)
    e_k = [
        selection(128, 256, lambda r, c, g=g: (c % 128 >= 64) & (c % 128 < 96) & (r == 32 * g + c % 128 - 64))
        for g in range(4)
    ]

    def build(d):
        piece = jnp.concatenate([msg[d, 0], msg[d, 1]], axis=0)
        lat, pk = piece[:T], piece[T:]
        pk = jnp.concatenate([pk[:, :128], pk[:, 128:]], axis=0)
        for g in range(4):
            k = mm(lat[128 * g : 128 * (g + 1)], ku2[...]) + mm(pk, e_k[g])
            kall[pl.ds(d * T + 128 * g, 128), :] = k.astype(BF16)
        v = lax.dot_general(vu_t, lat, (((1,), (1,)), ((), ())), preferred_element_type=F32).astype(BF16)
        for h in range(2):
            vt[h, pl.ds(0, VDIM), pl.ds(d * T, T)] = v[VDIM * h : VDIM * (h + 1)]

    build(0)

    swaps = {}
    for step in range(1, 4):
        zr_a.wait_recv()
        nr_a = key_send(step, s0, True)
        zl_b.wait_recv()
        nl_b = key_send(step, s1, False)
        zr_b.wait_recv()
        zl_a.wait_recv()
        if step < 3:
            nr_b, nl_a = key_send(step, s1, True), key_send(step, s0, False)
        for d in (step, NZ - step):
            swaps[d] = remote(msg.at[d, core], msg.at[d, core], partner)
        if step == 1:
            qr0.wait_recv()
            qr2 = remote(qs.at[1, 0, q96], qs.at[3, 0, q96], yr)
            ql0.wait_recv()
            ql2 = remote(qs.at[2, 1, q96], qs.at[3, 1, q96], yl)
        else:
            for d in (step - 1, NZ - step + 1):
                swaps[d].wait_recv()
                build(d)
        zr_a, zl_b = nr_a, nl_b
        if step < 3:
            zr_b, zl_a = nr_b, nl_a
    for d in (3, 5):
        swaps[d].wait_recv()
        build(d)
    zr_a.wait_recv()
    zl_b.wait_recv()
    swaps[4] = remote(msg.at[4, core], msg.at[4, core], partner)

    to_next.wait_recv()
    to_prev.wait_recv()
    cp = cprod[...].astype(F32)
    row = iota((T, 128), 0)
    before = jnp.where(sp > 0, halo[0].astype(F32)[15:16], 0.0)
    after = jnp.where(sp < NY * NZ - 1, halo[1].astype(F32)[0:1], 0.0)
    tap = taps[...].astype(F32)
    mixed = (
        jnp.where(row == 0, before, pltpu.roll(cp, 1, 0)) * tap[0:1]
        + cp * tap[1:2]
        + jnp.where(row == T - 1, after, pltpu.roll(cp, T - 1, 0)) * tap[2:3]
    )
    conv_out[...] = (silu(rounded(3)) * rounded(2) * mixed).astype(BF16)
    gate = silu(rounded(4))

    swaps[4].wait_recv()
    build(4)
    for c in (qr1, ql1, qr2, ql2):
        c.wait_recv()

    def stage(new, old, m_old):
        def body(j, mx):
            keys = pl.ds(pl.multiple_of(j * CHUNK, CHUNK), CHUNK)
            if new is not None:
                i, h = new
                s = mm(kall[keys, 128 * h : 128 * (h + 1)], qs[i, h])
                sbuf[h, keys, :] = s
                mx = jnp.maximum(mx, jnp.max(s.reshape(CHUNK // 8, 8, T), axis=0))
            if old is not None:
                g = old[1]
                p = jnp.exp2(sbuf[g, keys, :] - m_old).astype(BF16)
                acc[...] += mm(vt[g, :, keys], p)
            return mx

        if old is not None:
            acc[...] = jnp.zeros_like(acc)
        mx = lax.fori_loop(0, KEYS // CHUNK, body, jnp.full((8, T), -jnp.inf, F32))
        return jnp.max(mx, axis=0, keepdims=True)

    def finish(unit, m):
        i, h = unit
        total = acc[pl.ds(VDIM, 1), :]
        om[i, h] = (acc[pl.ds(0, VDIM), :] * (1.0 / total)).astype(BF16)
        ostat[i, h] = jnp.where(iota((8, T), 0) == 0, m, total)

    units = [(i, h) for i in (3, 2, 1, 0) for h in range(2)]
    back = {}
    m_now = stage(units[0], None, None)
    for n, unit in enumerate(units):
        following = units[n + 1] if n + 1 < len(units) else None
        m_next = stage(following, unit, m_now)
        finish(unit, m_now)
        m_now = m_next
        i, h = unit
        if i == 3:
            to = xr_y = yr if h == 0 else yl
            back[unit] = (remote(om.at[i, h], relay.at[h], to), remote(ostat.at[i, h], relay_stat.at[h], to))
        elif i in (1, 2):
            to, slot = (yl, 2) if i == 1 else (yr, 1)
            back[unit] = (remote(om.at[i, h], ro.at[slot, h], to), remote(ostat.at[i, h], rstat.at[slot, h], to))
        if i == 2:
            for c in back[(3, h)]:
                c.wait_recv()
            to = yr if h == 0 else yl
            back[(0, h)] = (remote(relay.at[h], ro.at[3, h], to), remote(relay_stat.at[h], rstat.at[3, h], to))
    for cs in [v for k, v in back.items() if k[0] != 3]:
        for c in cs:
            c.wait_recv()
    parts = []
    for h in range(2):
        os = [om[0, h]] + [ro[k, h] for k in (1, 2, 3)]
        st = [ostat[0, h]] + [rstat[k, h] for k in (1, 2, 3)]
        top = st[0][0:1]
        for s in st[1:]:
            top = jnp.maximum(top, s[0:1])
        weights = [s[1:2] * jnp.exp2(s[0:1] - top) for s in st]
        total = weights[0] + weights[1] + weights[2] + weights[3]
        summed = os[0].astype(F32) * weights[0]
        for o, w in zip(os[1:], weights[1:]):
            summed = summed + o.astype(F32) * w
        parts.append(summed / total)
    attended = jnp.transpose(jnp.concatenate(parts, axis=0))
    attn_out = (gate * attended).astype(BF16)
    for chip in range(NX):
        for c in range(2):
            rows = slice(128 * chip + 64 * c, 128 * chip + 64 * (c + 1))
            lhs[chip, c, :, pl.ds(0, 128)] = conv_out[rows, :]
            lhs[chip, c, :, pl.ds(128, 128)] = attn_out[rows]

    order = (2, 1, 3, 0)
    to_partner = {}
    for r in order:
        p_send[r] = mm(lhs[(x + r) % NX, other], wd[...]).astype(BF16)
        to_partner[r] = remote(p_send.at[r], p_recv.at[r], partner)
    for r in order:
        own[r] = mm(lhs[(x + r) % NX, core], wd[...])
    lo, hi = slice(0, 1024), slice(1024, 2048)
    to_partner[2].wait_recv()
    for k, cols in enumerate((lo, hi)):
        pair2[k] = (own[2, :, cols] + p_recv[2, :, cols].astype(F32)).astype(BF16)
    ta = remote(pair2.at[0], turn_a, xr)
    tb = remote(pair2.at[1], turn_b, xl)
    to_partner[1].wait_recv()
    pair1[1] = (own[1, :, hi] + p_recv[1, :, hi].astype(F32)).astype(BF16)
    far_r = remote(pair1.at[1], from_l.at[1], xr)
    to_partner[3].wait_recv()
    pair3[0] = (own[3, :, lo] + p_recv[3, :, lo].astype(F32)).astype(BF16)
    far_l = remote(pair3.at[0], from_r.at[0], xl)
    ta.wait_recv()
    pair1[0] = (own[1, :, lo] + p_recv[1, :, lo].astype(F32) + turn_a[...].astype(F32)).astype(BF16)
    near_r = remote(pair1.at[0], from_l.at[0], xr)
    tb.wait_recv()
    pair3[1] = (own[3, :, hi] + p_recv[3, :, hi].astype(F32) + turn_b[...].astype(F32)).astype(BF16)
    near_l = remote(pair3.at[1], from_r.at[1], xl)
    to_partner[0].wait_recv()
    far_r.wait_recv()
    far_l.wait_recv()
    near_r.wait_recv()
    near_l.wait_recv()
    for k, cols in enumerate((lo, hi)):
        out[:, cols] = (
            own[0, :, cols] + p_recv[0, :, cols].astype(F32) + from_l[k].astype(F32) + from_r[k].astype(F32)
        ).astype(BF16)
    for c in started:
        c.wait_send()


def scratch():
    v = lambda shape, kind=BF16: pltpu.VMEM(shape, kind)
    return [
        v((8, T, FB)), v((D, 640)), v((D, 192)), v((D, 256)), v((D, 256)), v((D, 32)), v((D, 128)),
        v((256, 128)), v((256, 256)), v((256, 128)), v((256, D)), v((3, 128)), v((256,), F32),
        v((T, 640), F32), v((T, 256), F32), v((T, 256), F32), v((T, 128), F32), v((T, 128), F32),
        v((T, 128), F32), v((T, 128), F32),
        v((NZ, 2, HALF, 256)), v((NY, 2, 128, T)), v((KEYS, 256)), v((2, VROWS, KEYS)),
        v((2, KEYS, T), F32), v((VROWS, T), F32),
        v((NY, 2, VDIM, T)), v((NY, 2, 8, T), F32), v((NY, 2, VDIM, T)), v((NY, 2, 8, T), F32),
        v((2, VDIM, T)), v((2, 8, T), F32),
        v((T, 128)), v((2, 16, 128)), v((T, 128)), v((NX, 2, 64, 256)),
        v((NX, 64, D)), v((NX, 64, D)), v((NX, 64, D), F32),
        v((2, 64, 1024)), v((2, 64, 1024)), v((2, 64, 1024)), v((64, 1024)), v((64, 1024)),
        v((2, 64, 1024)), v((2, 64, 1024)),
        pltpu.SemaphoreType.DMA((N_REMOTE,)), pltpu.SemaphoreType.DMA((N_REMOTE,)),
        pltpu.SemaphoreType.DMA((N_LOCAL,)),
    ]


def on_device(*args):
    return pl.pallas_call(
        layer_kernel,
        out_shape=jax.ShapeDtypeStruct((64, D), BF16),
        in_specs=[pl.BlockSpec(memory_space=pl.ANY)] * len(args),
        out_specs=pl.BlockSpec(memory_space=pltpu.VMEM),
        scratch_shapes=scratch(),
        compiler_params=pltpu.CompilerParams(
            collective_id=0, has_side_effects=True, vmem_limit_bytes=62 * 1024 * 1024
        ),
        name="layer",
    )(*args)


def solution(mesh):
    cols, rows, whole = P(None, "tp"), P("tp", None), P()
    placed = (P("sp", "tp"), cols, cols, cols, cols, cols, cols, whole, whole, whole, cols, cols, cols, rows, rows)
    return jax.shard_map(
        on_device, mesh=mesh, in_specs=placed, out_specs=P(("sp", "tp"), None), check_vma=False
    )
```

```python
import math

import jax
import jax.numpy as jnp
from jax import lax
from jax.experimental import pallas as pl
from jax.experimental.pallas import tpu as pltpu
from jax.sharding import PartitionSpec as P

NOPE, ROPE, VDIM, GRID_W = 64, 32, 64, 64
EPS = 1e-06
THETA = 10000.0
D = 2048
T = 512
FB = 256
NX, NY, NZ = 4, 4, 8
KEYS = NZ * T
PIECE = T + 64
HALF = PIECE // 2
SUB = HALF // 2
VROWS = VDIM + 16
CHUNK = 512
ARRIVAL = (0, 1, 7, 2, 6, 3, 5, 4)
N_REMOTE = 96
N_LOCAL = 16
MESH = pl.DeviceIdType.MESH
F32, BF16 = jnp.float32, jnp.bfloat16


def iota(shape, dim):
    return lax.broadcasted_iota(jnp.int32, shape, dim)


def mm(a, b):
    return jnp.dot(a, b, preferred_element_type=F32)


def silu(v):
    return v * (1.0 / (1.0 + jnp.exp(-v)))


def selection(rows, cols, test):
    return jnp.where(test(iota((rows, cols), 0), iota((rows, cols), 1)), 1.0, 0.0).astype(BF16)


def layer_kernel(
    tokens, conv_input, conv_inner, conv_outer, conv_gate, conv_taps, query_proj, latent_proj,
    rope_proj, latent_gain, key_up, value_up, attn_gate, conv_down, attn_down,
    out,
    xall, w5, wqr, wl, ku_raw, ku2, vu_raw, wd, taps, gain,
    a5, al, aqr, ss,
    msg, qs, kall, vt, sbuf, acc, tops,
    om, ostat, ro, rstat, relay, relay_stat, both, both_stat,
    wall, aout, aall, cprod, halo, conv_out, gate_out, p_send, p_recv, own, pair2, pair1, pair3, turn_a, turn_b, from_l, from_r,
    send_sems, recv_sems, local_sems,
):
    sp, tp = lax.axis_index("sp"), lax.axis_index("tp")
    z, y = sp // NY, sp % NY
    x, core = tp // 2, tp % 2
    other = 1 - core
    dev = lambda s, t: {"sp": s, "tp": t}
    partner = dev(sp, x * 2 + other)
    xr, xl = dev(sp, (x + 1) % NX * 2 + core), dev(sp, (x + NX - 1) % NX * 2 + core)
    yr, yl = dev(z * NY + (y + 1) % NY, tp), dev(z * NY + (y + NY - 1) % NY, tp)
    zr, zl = dev((z + 1) % NZ * NY + y, tp), dev((z + NZ - 1) % NZ * NY + y, tp)
    span_next, span_prev = dev((sp + 1) % (NZ * NY), tp), dev((sp + NZ * NY - 1) % (NZ * NY), tp)

    started = []

    def remote(src, dst, to):
        k = len(started)
        copy = pltpu.make_async_remote_copy(
            src_ref=src, dst_ref=dst, send_sem=send_sems.at[k], recv_sem=recv_sems.at[k],
            device_id=to, device_id_type=MESH,
        )
        copy.start()
        started.append(copy)
        return copy

    locals_ = []

    def load(src, dst):
        copy = pltpu.make_async_copy(src, dst, local_sems.at[len(locals_)])
        copy.start()
        locals_.append(copy)
        return copy

    own_block = load(tokens, xall.at[0])
    loads_proj = [load(query_proj, wqr.at[pl.ds(0, 192), :]), load(rope_proj, wqr.at[pl.ds(192, ROPE), :])]
    loads_proj += [
        load(w, w5.at[:, pl.ds(128 * k, 128)])
        for k, w in enumerate((conv_input, conv_inner, conv_outer, conv_gate, attn_gate))
    ]
    loads_proj.append(load(latent_proj, wl))
    loads_late = [load(conv_taps, taps), load(latent_gain, gain), load(key_up, ku_raw), load(value_up, vu_raw)]
    loads_late += [load(conv_down, wd), load(attn_down, wall.at[0, 0])]

    barrier = pltpu.get_barrier_semaphore()
    tp_peer = lambda r, c: dev(sp, (x + r) % NX * 2 + c)
    peers = [tp_peer(r, c) for r in (1, 2, 3) for c in (core, other)]
    peers += [partner, yr, yl, zr, zl, span_next, span_prev]
    for to in peers:
        pl.semaphore_signal(barrier, inc=1, device_id=to, device_id_type=MESH)
    pl.semaphore_wait(barrier, len(peers))

    own_block.wait()
    h0, h1 = pl.ds(0, T // 2), pl.ds(T // 2, T // 2)
    r0 = remote(xall.at[0, h0], xall.at[1, h0], xr)
    l0 = remote(xall.at[0, h1], xall.at[2, h1], xl)
    r1 = remote(xall.at[0, h1], xall.at[1, h1], xr)
    l1 = remote(xall.at[0, h0], xall.at[2, h0], xl)
    d0 = remote(xall.at[0], xall.at[4], partner)

    token = iota((8, T), 1) + sp * T
    entry = iota((8, T), 0)
    freq = jnp.zeros((8, T), F32)
    for j in range(8):
        freq = jnp.where(entry == j, float(THETA ** (-2.0 * j / 16)), freq)
    row_angle = (token // GRID_W).astype(F32) * freq
    col_angle = (token % GRID_W).astype(F32) * freq
    tables = (jnp.cos(row_angle), jnp.sin(row_angle), jnp.cos(col_angle), jnp.sin(col_angle))
    for i in range(NY):
        for h in range(2):
            qs[i, h, pl.ds(96, 32), :] = jnp.zeros((32, T), BF16)
    for h in range(2):
        vt[h, pl.ds(VDIM, 16), :] = jnp.where(iota((16, KEYS), 0) == 0, 1.0, 0.0).astype(BF16)
    for c in loads_proj:
        c.wait()

    def project(slot, chip, c, first=False):
        block = pl.multiple_of((chip * 2 + c) * FB, FB)

        def rows_of(i, _):
            rows = pl.ds(pl.multiple_of(i * 256, 256), 256)
            v = xall[slot, rows, :]
            wide = v.astype(F32)
            squares = wide[:, :128] * wide[:, :128] + wide[:, 128:] * wide[:, 128:]
            for total, w in ((a5, w5), (al, wl)):
                term = mm(v, w[pl.ds(block, FB), :])
                total[rows, :] = term if first else total[rows, :] + term
            term = lax.dot_general(
                wqr[:, pl.ds(block, FB)], v, (((1,), (1,)), ((), ())), preferred_element_type=F32
            )
            aqr[:, rows] = term if first else aqr[:, rows] + term
            ss[rows, :] = squares if first else ss[rows, :] + squares
            return 0

        lax.fori_loop(0, T // 256, rows_of, 0)

    left, right, across = (x + NX - 1) % NX, (x + 1) % NX, (x + 2) % NX
    r0.wait_recv()
    r2 = remote(xall.at[1, h0], xall.at[3, h0], xr)
    l0.wait_recv()
    l2 = remote(xall.at[2, h1], xall.at[3, h1], xl)
    project(0, x, core, first=True)
    d0.wait_recv()
    project(4, x, other)
    r1.wait_recv()
    d1 = remote(xall.at[1], xall.at[5], partner)
    l1.wait_recv()
    d2 = remote(xall.at[2], xall.at[6], partner)
    project(1, left, core)
    project(2, right, core)
    d1.wait_recv()
    project(5, left, other)
    r2.wait_recv()
    d3a = remote(xall.at[3, h0], xall.at[7, h0], partner)
    l2.wait_recv()
    d3b = remote(xall.at[3, h1], xall.at[7, h1], partner)
    d2.wait_recv()
    project(6, right, other)
    project(3, across, core)
    d3a.wait_recv()
    d3b.wait_recv()
    project(7, across, other)
    for c in loads_late:
        c.wait()

    scale = lax.rsqrt(jnp.sum(ss[...], axis=1, keepdims=True) / D + EPS)
    zl_ = al[...] * scale
    latent = zl_ * lax.rsqrt(jnp.mean(zl_ * zl_, axis=1, keepdims=True) + EPS) * gain[...].reshape(1, 256)
    latent = latent.astype(BF16)
    msg[0, 0] = latent[:HALF]
    msg[0, 1, pl.ds(0, T - HALF), :] = latent[HALF:]

    def turned(v):
        a, b, c, d = v[0:8], v[8:16], v[16:24], v[24:32]
        cos_r, sin_r, cos_c, sin_c = tables
        return jnp.concatenate(
            [a * cos_r - b * sin_r, b * cos_r + a * sin_r, c * cos_c - d * sin_c, d * cos_c + c * sin_c], axis=0
        )

    scale_row = lax.rsqrt(jnp.sum(jnp.transpose(ss[...]), axis=0, keepdims=True) / D + EPS)
    key_rope = turned(aqr[pl.ds(192, ROPE), :] * scale_row).astype(BF16)
    msg[0, 1, pl.ds(T - HALF, ROPE), :] = key_rope[:, :256]
    msg[0, 1, pl.ds(T - HALF + ROPE, ROPE), :] = key_rope[:, 256:]

    s0, s1 = pl.ds(0, SUB), pl.ds(SUB, SUB)

    def key_send(step, sub, to_right):
        d_from, d_to = (step, step + 1) if to_right else ((NZ - step) % NZ, NZ - 1 - step)
        return remote(msg.at[d_from, core, sub], msg.at[d_to, core, sub], zr if to_right else zl)

    zr_a, zl_b = key_send(0, s0, True), key_send(0, s1, False)
    zr_b, zl_a = key_send(0, s1, True), key_send(0, s0, False)

    rounded = lambda k: (a5[:, 128 * k : 128 * (k + 1)] * scale).astype(BF16).astype(F32)
    cprod[...] = (rounded(1) * rounded(0)).astype(BF16)
    to_next = remote(cprod.at[pl.ds(T - 16, 16)], halo.at[0], span_next)
    to_prev = remote(cprod.at[pl.ds(0, 16)], halo.at[1], span_prev)

    q_scale = scale_row * ((NOPE + ROPE) ** (-0.5) * math.log2(math.e))
    for h in range(2):
        qs[0, h, pl.ds(0, NOPE), :] = (aqr[pl.ds(96 * h, NOPE), :] * q_scale).astype(BF16)
        qs[0, h, pl.ds(NOPE, ROPE), :] = turned(aqr[pl.ds(96 * h + NOPE, ROPE), :] * q_scale).astype(BF16)
    q96 = pl.ds(0, 96)
    qr0 = remote(qs.at[0, 0, q96], qs.at[1, 0, q96], yr)
    ql0 = remote(qs.at[0, 1, q96], qs.at[2, 1, q96], yl)
    qr1 = remote(qs.at[0, 1, q96], qs.at[1, 1, q96], yr)
    ql1 = remote(qs.at[0, 0, q96], qs.at[2, 0, q96], yl)

    w0, w1 = pl.ds(0, 64), pl.ds(64, 64)
    wr0 = remote(wall.at[0, 0, w0], wall.at[1, 0, w0], xr)
    wl0 = remote(wall.at[0, 0, w1], wall.at[2, 0, w1], xl)
    wr1 = remote(wall.at[0, 0, w1], wall.at[1, 0, w1], xr)
    wl1 = remote(wall.at[0, 0, w0], wall.at[2, 0, w0], xl)
    wd0 = remote(wall.at[0, 0], wall.at[0, 1], partner)

    ku2[...] = mm(
        ku_raw[...], selection(128, 256, lambda r, c: (c % 128 < 64) & (r == c // 128 * 64 + c % 128))
    ).astype(BF16)
    vu_t = jnp.transpose(vu_raw[...].astype(F32)).astype(BF16)
    e_k = selection(ROPE, 256, lambda r, c: (c % 128 >= 64) & (c % 128 < 96) & (r == c % 128 - 64))
    place = {d: n * T for n, d in enumerate(ARRIVAL)}

    def build(d):
        piece = jnp.concatenate([msg[d, 0], msg[d, 1]], axis=0)
        lat = piece[:T]
        for g in range(2):
            pk = jnp.transpose(piece[T + ROPE * g : T + ROPE * (g + 1)].astype(F32)).astype(BF16)
            k = mm(lat[256 * g : 256 * (g + 1)], ku2[...]) + mm(pk, e_k)
            kall[pl.ds(place[d] + 256 * g, 256), :] = k.astype(BF16)
        v = lax.dot_general(vu_t, lat, (((1,), (1,)), ((), ())), preferred_element_type=F32).astype(BF16)
        for h in range(2):
            vt[h, pl.ds(0, VDIM), pl.ds(place[d], T)] = v[VDIM * h : VDIM * (h + 1)]

    build(0)

    right_a, left_b, right_b, left_a, swaps = {0: zr_a}, {0: zl_b}, {0: zr_b}, {0: zl_a}, {}

    def step_a(step):
        right_a[step - 1].wait_recv()
        if step < 4:
            right_a[step] = key_send(step, s0, True)
        left_b[step - 1].wait_recv()
        if step < 4:
            left_b[step] = key_send(step, s1, False)
        else:
            swaps[4] = remote(msg.at[4, core], msg.at[4, core], partner)

    def step_b(step):
        right_b[step - 1].wait_recv()
        if step < 3:
            right_b[step] = key_send(step, s1, True)
        left_a[step - 1].wait_recv()
        if step < 3:
            left_a[step] = key_send(step, s0, False)
        for d in (step, NZ - step):
            swaps[d] = remote(msg.at[d, core], msg.at[d, core], partner)

    def arrive(*pieces):
        for d in pieces:
            swaps[d].wait_recv()
            build(d)

    groups = ((0, 3), (3, 2), (5, 3))

    def stage(new, old, top_old):
        top_new = None
        if new is not None:
            (first, count), i, h = groups[new[0]], new[1], new[2]
            mx = None
            for j in range(count * T // CHUNK):
                s = mm(kall[pl.ds(first * T + j * CHUNK, CHUNK), 128 * h : 128 * (h + 1)], qs[i, h])
                sbuf[h, pl.ds(j * CHUNK, CHUNK), :] = s
                m = jnp.max(s.reshape(CHUNK // 8, 8, T), axis=0)
                mx = m if mx is None else jnp.maximum(mx, m)
            top_new = jnp.max(mx, axis=0, keepdims=True)
        if old is not None:
            (first, count), i, h = groups[old[0]], old[1], old[2]
            if old[0] > 0:
                before = tops[i, h, pl.ds(0, 1), :]
                top_old = jnp.maximum(before, top_old)
            total = None
            for j in range(count * T // CHUNK):
                p = jnp.exp2(sbuf[h, pl.ds(j * CHUNK, CHUNK), :] - top_old).astype(BF16)
                term = mm(vt[h, :, pl.ds(first * T + j * CHUNK, CHUNK)], p)
                total = term if total is None else total + term
            if old[0] > 0:
                total = total + acc[i, h] * jnp.exp2(before - top_old)
            acc[i, h] = total
            tops[i, h] = jnp.broadcast_to(top_old, (8, T))
        return top_new

    def finish(i, h):
        total = acc[i, h, pl.ds(VDIM, 1), :]
        om[i, h] = (acc[i, h, pl.ds(0, VDIM), :] * (1.0 / total)).astype(BF16)
        ostat[i, h] = jnp.concatenate([tops[i, h, pl.ds(0, 1), :], total], axis=0)

    def merged(parts):
        parts = [(o[...].astype(F32), st[...]) for o, st in parts]
        top = parts[0][1][0:1]
        for _, st in parts[1:]:
            top = jnp.maximum(top, st[0:1])
        weights = [st[1:2] * jnp.exp2(st[0:1] - top) for _, st in parts]
        total, summed = weights[0], parts[0][0] * weights[0]
        for w, (o, _) in zip(weights[1:], parts[1:]):
            total, summed = total + w, summed + o * w
        return summed / total, jnp.concatenate([top, total], axis=0)

    lo, hi = slice(0, 1024), slice(1024, 2048)
    order = (2, 1, 3, 0)
    sums = {}

    def conv_rows(r, c):
        return conv_out[pl.ds(pl.multiple_of((x + r) % NX * 128 + c * 64, 64), 64), :]

    def conv_partials():
        for r in order:
            p_send[r] = mm(conv_rows(r, other), wd[...]).astype(BF16)
            sums[r] = remote(p_send.at[r], p_recv.at[r], partner)
        for r in order:
            own[r] = mm(conv_rows(r, core), wd[...])

    def conv_first():
        sums[2].wait_recv()
        for k, cols in enumerate((lo, hi)):
            pair2[k] = (own[2, :, cols] + p_recv[2, :, cols].astype(F32)).astype(BF16)
        sums["a"] = remote(pair2.at[0], turn_a, xr)
        sums["b"] = remote(pair2.at[1], turn_b, xl)
        sums[1].wait_recv()
        pair1[1] = (own[1, :, hi] + p_recv[1, :, hi].astype(F32)).astype(BF16)
        sums["far_r"] = remote(pair1.at[1], from_l.at[1], xr)
        sums[3].wait_recv()
        pair3[0] = (own[3, :, lo] + p_recv[3, :, lo].astype(F32)).astype(BF16)
        sums["far_l"] = remote(pair3.at[0], from_r.at[0], xl)

    def conv_second():
        sums["a"].wait_recv()
        pair1[0] = (own[1, :, lo] + p_recv[1, :, lo].astype(F32) + turn_a[...].astype(F32)).astype(BF16)
        sums["near_r"] = remote(pair1.at[0], from_l.at[0], xr)
        sums["b"].wait_recv()
        pair3[1] = (own[3, :, hi] + p_recv[3, :, hi].astype(F32) + turn_b[...].astype(F32)).astype(BF16)
        sums["near_l"] = remote(pair3.at[1], from_r.at[1], xl)

    weight_hops = {}

    def weights_on(k):
        if k == 0:
            wr0.wait_recv()
            weight_hops["r"] = remote(wall.at[1, 0, w0], wall.at[3, 0, w0], xr)
            wl0.wait_recv()
            weight_hops["l"] = remote(wall.at[2, 0, w1], wall.at[3, 0, w1], xl)
        elif k == 1:
            wr1.wait_recv()
            weight_hops[1] = remote(wall.at[1, 0], wall.at[1, 1], partner)
            wl1.wait_recv()
            weight_hops[2] = remote(wall.at[2, 0], wall.at[2, 1], partner)
        else:
            weight_hops["r"].wait_recv()
            weight_hops["l"].wait_recv()
            weight_hops[3] = remote(wall.at[3, 0], wall.at[3, 1], partner)

    step_a(1)
    step_b(1)
    qr0.wait_recv()
    qr2 = remote(qs.at[1, 0, q96], qs.at[3, 0, q96], yr)
    ql0.wait_recv()
    ql2 = remote(qs.at[2, 1, q96], qs.at[3, 1, q96], yl)
    to_next.wait_recv()
    to_prev.wait_recv()
    cp = cprod[...].astype(F32)
    row = iota((T, 128), 0)
    before = jnp.where(sp > 0, halo[0].astype(F32)[15:16], 0.0)
    after = jnp.where(sp < NY * NZ - 1, halo[1].astype(F32)[0:1], 0.0)
    tap = taps[...].astype(F32)
    mixed = (
        jnp.where(row == 0, before, pltpu.roll(cp, 1, 0)) * tap[0:1]
        + cp * tap[1:2]
        + jnp.where(row == T - 1, after, pltpu.roll(cp, T - 1, 0)) * tap[2:3]
    )
    conv_out[...] = (silu(rounded(3)) * rounded(2) * mixed).astype(BF16)
    gate_out[...] = silu(rounded(4))
    arrive(1, 7)

    def key_events(n):
        if n == 0:
            step_a(2)
        elif n == 1:
            weights_on(0)
        elif n == 2:
            qr1.wait_recv()
            ql1.wait_recv()
        elif n == 3:
            step_b(2)
        elif n == 5:
            step_a(3)
            qr2.wait_recv()
            ql2.wait_recv()
        elif n == 7:
            arrive(2, 6)
        elif n == 8:
            step_b(3)
            weights_on(1)
        elif n == 9:
            conv_partials()
        elif n == 12:
            step_a(4)
            conv_first()
        elif n == 13:
            arrive(3, 5, 4)
        elif n == 16:
            weights_on(2)
        elif n == 19:
            conv_second()

    units = [(0, i, h) for i in (0, 1, 2, 3) for h in range(2)]
    units += [(g, i, h) for g in (1, 2) for i in (3, 2, 1) for h in range(2)]
    units += [(g, 0, h) for g in (1, 2) for h in range(2)]
    back = {}
    top = stage(units[0], None, None)
    for n, (group, i, h) in enumerate(units):
        key_events(n)
        unit = (i, h)
        top = stage(units[n + 1] if n + 1 < len(units) else None, units[n], top)
        if group < 2:
            continue
        finish(i, h)
        if i == 3:
            to = yr if h == 0 else yl
            back[unit] = (remote(om.at[i, h], relay.at[h], to), remote(ostat.at[i, h], relay_stat.at[h], to))
        elif unit == (2, 1):
            back["l", 1] = (remote(om.at[2, 1], ro.at[0, 1], yr), remote(ostat.at[2, 1], rstat.at[0, 1], yr))
        elif unit == (1, 0):
            back["r", 0] = (remote(om.at[1, 0], ro.at[1, 0], yl), remote(ostat.at[1, 0], rstat.at[1, 0], yl))
        elif unit == (1, 1):
            for k, i2, to, side in ((0, 2, yr, "l"), (1, 1, yl, "r")):
                for c in back[(3, k)]:
                    c.wait_recv()
                o, st = merged([(om.at[i2, k], ostat.at[i2, k]), (relay.at[k], relay_stat.at[k])])
                both[k] = o.astype(BF16)
                both_stat[k] = st
                slot = 0 if side == "l" else 1
                back[side, k] = (
                    remote(both.at[k], ro.at[slot, k], to), remote(both_stat.at[k], rstat.at[slot, k], to)
                )
    for side in "lr":
        for k in range(2):
            for c in back[side, k]:
                c.wait_recv()
    parts = [
        merged([(om.at[0, h], ostat.at[0, h])] + [(ro.at[k, h], rstat.at[k, h]) for k in range(2)])[0]
        for h in range(2)
    ]
    attended = jnp.transpose(jnp.concatenate(parts, axis=0))
    aout[...] = (gate_out[...] * attended).astype(BF16)

    def tile(r, c):
        return aout.at[pl.ds(pl.multiple_of((x + r) % NX * 128 + c * 64, 64), 64)]

    tiles = []
    for r, slot in ((2, 3), (1, 1), (3, 2), (0, 0)):
        for k, c in enumerate((core, other)):
            if r or k:
                tiles.append(remote(tile(r, c), aall.at[slot, k], tp_peer(r, c) if r else partner))
    aall[0, 0] = tile(0, core)[...]
    for k in (0, "far_r", "far_l", "near_r", "near_l"):
        sums[k].wait_recv()
    for k, cols in enumerate((lo, hi)):
        own[0, :, cols] = (
            own[0, :, cols] + p_recv[0, :, cols].astype(F32) + from_l[k].astype(F32) + from_r[k].astype(F32)
        )
    wd0.wait_recv()
    for k in (1, 2, 3):
        weight_hops[k].wait_recv()
    for c in tiles:
        c.wait_recv()
    rows = jnp.concatenate([aall[s, k] for s in range(NX) for k in range(2)], axis=1)
    for n in range(4):
        cols = pl.ds(512 * n, 512)
        term = own[0, :, cols]
        for s in range(NX):
            w = jnp.concatenate([wall[s, 0, :, cols], wall[s, 1, :, cols]], axis=0)
            term = term + mm(rows[:, 256 * s : 256 * (s + 1)], w)
        out[:, cols] = term.astype(BF16)
    for c in started:
        c.wait_send()


def scratch():
    v = lambda shape, kind=BF16: pltpu.VMEM(shape, kind)
    return [
        v((8, T, FB)), v((D, 640)), v((224, D)), v((D, 256)),
        v((256, 128)), v((256, 256)), v((256, 128)), v((128, D)), v((3, 128)), v((256,), F32),
        v((T, 640), F32), v((T, 256), F32), v((224, T), F32), v((T, 128), F32),
        v((NZ, 2, HALF, 256)), v((NY, 2, 128, T)), v((KEYS, 256)), v((2, VROWS, KEYS)),
        v((2, 3 * T, T), F32), v((NY, 2, VROWS, T), F32), v((NY, 2, 8, T), F32),
        v((NY, 2, VDIM, T)), v((NY, 2, 2, T), F32), v((2, 2, VDIM, T)), v((2, 2, 2, T), F32),
        v((2, VDIM, T)), v((2, 2, T), F32), v((2, VDIM, T)), v((2, 2, T), F32),
        v((NX, 2, 128, D)), v((T, 128)), v((NX, 2, 64, 128)),
        v((T, 128)), v((2, 16, 128)), v((T, 128)), v((T, 128), F32),
        v((NX, 64, D)), v((NX, 64, D)), v((NX, 64, D), F32),
        v((2, 64, 1024)), v((2, 64, 1024)), v((2, 64, 1024)), v((64, 1024)), v((64, 1024)),
        v((2, 64, 1024)), v((2, 64, 1024)),
        pltpu.SemaphoreType.DMA((N_REMOTE,)), pltpu.SemaphoreType.DMA((N_REMOTE,)),
        pltpu.SemaphoreType.DMA((N_LOCAL,)),
    ]


def on_device(*args):
    args = tuple(a.T if k in (6, 8) else a for k, a in enumerate(args))
    return pl.pallas_call(
        layer_kernel,
        out_shape=jax.ShapeDtypeStruct((64, D), BF16),
        in_specs=[pl.BlockSpec(memory_space=pl.ANY)] * len(args),
        out_specs=pl.BlockSpec(memory_space=pltpu.VMEM),
        scratch_shapes=scratch(),
        compiler_params=pltpu.CompilerParams(
            collective_id=0, has_side_effects=True, vmem_limit_bytes=62 * 1024 * 1024
        ),
        name="layer",
    )(*args)


def solution(mesh):
    cols, rows, whole = P(None, "tp"), P("tp", None), P()
    placed = (P("sp", "tp"), cols, cols, cols, cols, cols, cols, whole, whole, whole, cols, cols, cols, rows, rows)
    return jax.shard_map(
        on_device, mesh=mesh, in_specs=placed, out_specs=P(("sp", "tp"), None), check_vma=False
    )
```

```python
import math

import jax
import jax.numpy as jnp
from jax import lax
from jax.experimental import pallas as pl
from jax.experimental.pallas import tpu as pltpu
from jax.sharding import PartitionSpec as P

NOPE, ROPE, VDIM, GRID_W = 64, 32, 64, 64
EPS = 1e-06
THETA = 10000.0
D = 2048
T = 512
FB = 256
NX, NY, NZ = 4, 4, 8
KEYS = NZ * T
PIECE = T + 64
HALF = PIECE // 2
SUB = HALF // 2
VROWS = VDIM + 16
CHUNK = 256
ARRIVAL = (0, 1, 7, 2, 6, 3, 5, 4)
N_REMOTE = 96
N_LOCAL = 16
MESH = pl.DeviceIdType.MESH
F32, BF16 = jnp.float32, jnp.bfloat16


def iota(shape, dim):
    return lax.broadcasted_iota(jnp.int32, shape, dim)


def mm(a, b):
    return jnp.dot(a, b, preferred_element_type=F32)


def silu(v):
    return v * (1.0 / (1.0 + jnp.exp(-v)))


def selection(rows, cols, test):
    return jnp.where(test(iota((rows, cols), 0), iota((rows, cols), 1)), 1.0, 0.0).astype(BF16)


def layer_kernel(
    tokens, conv_input, conv_inner, conv_outer, conv_gate, conv_taps, query_proj, latent_proj,
    rope_proj, latent_gain, key_up, value_up, attn_gate, conv_down, attn_down,
    out,
    xall, w5, wqr, wl, ku_raw, ku2, vu_raw, vu_t, e_k, wd, taps, gain,
    a5, al, aqr, ss,
    msg, qs, kall, vt, sbuf, acc, tops,
    om, ostat, ro, rstat, relay, relay_stat, both, both_stat,
    wall, aout, aall, cprod, halo, conv_out, gate_out, p_send, p_recv, own, pair2, pair1, pair3, turn_a, turn_b, from_l, from_r,
    send_sems, recv_sems, local_sems,
):
    sp, tp = lax.axis_index("sp"), lax.axis_index("tp")
    z, y = sp // NY, sp % NY
    x, core = tp // 2, tp % 2
    other = 1 - core
    dev = lambda s, t: {"sp": s, "tp": t}
    partner = dev(sp, x * 2 + other)
    xr, xl = dev(sp, (x + 1) % NX * 2 + core), dev(sp, (x + NX - 1) % NX * 2 + core)
    yr, yl = dev(z * NY + (y + 1) % NY, tp), dev(z * NY + (y + NY - 1) % NY, tp)
    zr, zl = dev((z + 1) % NZ * NY + y, tp), dev((z + NZ - 1) % NZ * NY + y, tp)
    span_next, span_prev = dev((sp + 1) % (NZ * NY), tp), dev((sp + NZ * NY - 1) % (NZ * NY), tp)

    started = []

    def remote(src, dst, to):
        k = len(started)
        copy = pltpu.make_async_remote_copy(
            src_ref=src, dst_ref=dst, send_sem=send_sems.at[k], recv_sem=recv_sems.at[k],
            device_id=to, device_id_type=MESH,
        )
        copy.start()
        started.append(copy)
        return copy

    locals_ = []

    def load(src, dst):
        copy = pltpu.make_async_copy(src, dst, local_sems.at[len(locals_)])
        copy.start()
        locals_.append(copy)
        return copy

    own_block = load(tokens, xall.at[0])
    loads_proj = [load(query_proj, wqr.at[pl.ds(0, 192), :]), load(rope_proj, wqr.at[pl.ds(192, ROPE), :])]
    loads_proj += [
        load(w, w5.at[:, pl.ds(128 * k, 128)])
        for k, w in enumerate((conv_input, conv_inner, conv_outer, conv_gate, attn_gate))
    ]
    loads_proj.append(load(latent_proj, wl))
    loads_late = [load(conv_taps, taps), load(latent_gain, gain)]
    loads_kv = [load(key_up, ku_raw), load(value_up, vu_raw)]
    loads_late += [load(conv_down, wd), load(attn_down, wall.at[0, 0])]

    barrier = pltpu.get_barrier_semaphore()
    tp_peer = lambda r, c: dev(sp, (x + r) % NX * 2 + c)
    peers = [tp_peer(r, c) for r in (1, 2, 3) for c in (core, other)]
    peers += [partner, yr, yl, zr, zl, span_next, span_prev]
    for to in peers:
        pl.semaphore_signal(barrier, inc=1, device_id=to, device_id_type=MESH)
    pl.semaphore_wait(barrier, len(peers))

    own_block.wait()
    h0, h1 = pl.ds(0, T // 2), pl.ds(T // 2, T // 2)
    r0 = remote(xall.at[0, h0], xall.at[1, h0], xr)
    l0 = remote(xall.at[0, h1], xall.at[2, h1], xl)
    r1 = remote(xall.at[0, h1], xall.at[1, h1], xr)
    l1 = remote(xall.at[0, h0], xall.at[2, h0], xl)
    d0 = remote(xall.at[0], xall.at[4], partner)

    token = iota((8, T), 1) + sp * T
    entry = iota((8, T), 0)
    freq = jnp.zeros((8, T), F32)
    for j in range(8):
        freq = jnp.where(entry == j, float(THETA ** (-2.0 * j / 16)), freq)
    row_angle = (token // GRID_W).astype(F32) * freq
    col_angle = (token % GRID_W).astype(F32) * freq
    tables = (jnp.cos(row_angle), jnp.sin(row_angle), jnp.cos(col_angle), jnp.sin(col_angle))
    for i in range(NY):
        for h in range(2):
            qs[i, h, pl.ds(96, 32), :] = jnp.zeros((32, T), BF16)
    for h in range(2):
        vt[h, pl.ds(VDIM, 16), :] = jnp.where(iota((16, KEYS), 0) == 0, 1.0, 0.0).astype(BF16)
    for c in loads_proj:
        c.wait()

    def project(slot, chip, c, first=False, early=True, late=True):
        block = pl.multiple_of((chip * 2 + c) * FB, FB)

        def rows_of(i, _):
            rows = pl.ds(pl.multiple_of(i * 256, 256), 256)
            v = xall[slot, rows, :]
            if early:
                wide = v.astype(F32)
                squares = wide[:, :128] * wide[:, :128] + wide[:, 128:] * wide[:, 128:]
                ss[rows, :] = squares if first else ss[rows, :] + squares
                term = lax.dot_general(
                    wqr[:, pl.ds(block, FB)], v, (((1,), (1,)), ((), ())), preferred_element_type=F32
                )
                aqr[:, rows] = term if first else aqr[:, rows] + term
            for total, w, now in ((al, wl, early), (a5, w5, late)):
                if now:
                    term = mm(v, w[pl.ds(block, FB), :])
                    total[rows, :] = term if first else total[rows, :] + term
            return 0

        lax.fori_loop(0, T // 256, rows_of, 0)

    left, right, across = (x + NX - 1) % NX, (x + 1) % NX, (x + 2) % NX
    r0.wait_recv()
    r2 = remote(xall.at[1, h0], xall.at[3, h0], xr)
    l0.wait_recv()
    l2 = remote(xall.at[2, h1], xall.at[3, h1], xl)
    project(0, x, core, first=True)
    d0.wait_recv()
    project(4, x, other)
    for c in loads_kv:
        c.wait()
    ku2[...] = mm(
        ku_raw[...], selection(128, 256, lambda r, c: (c % 128 < 64) & (r == c // 128 * 64 + c % 128))
    ).astype(BF16)
    vu_t[...] = jnp.transpose(vu_raw[...].astype(F32)).astype(BF16)
    e_k[...] = selection(ROPE, 256, lambda r, c: (c % 128 >= 64) & (c % 128 < 96) & (r == c % 128 - 64))
    r1.wait_recv()
    d1 = remote(xall.at[1], xall.at[5], partner)
    l1.wait_recv()
    d2 = remote(xall.at[2], xall.at[6], partner)
    project(1, left, core)
    project(2, right, core)
    d1.wait_recv()
    project(5, left, other)
    r2.wait_recv()
    d3a = remote(xall.at[3, h0], xall.at[7, h0], partner)
    l2.wait_recv()
    d3b = remote(xall.at[3, h1], xall.at[7, h1], partner)
    d2.wait_recv()
    project(6, right, other, late=False)
    project(3, across, core, late=False)
    d3a.wait_recv()
    d3b.wait_recv()
    project(7, across, other, late=False)
    for c in loads_late:
        c.wait()

    scale = lax.rsqrt(jnp.sum(ss[...], axis=1, keepdims=True) / D + EPS)
    zl_ = al[...] * scale
    latent = zl_ * lax.rsqrt(jnp.mean(zl_ * zl_, axis=1, keepdims=True) + EPS) * gain[...].reshape(1, 256)
    latent = latent.astype(BF16)
    msg[0, 0] = latent[:HALF]
    msg[0, 1, pl.ds(0, T - HALF), :] = latent[HALF:]

    def turned(v):
        a, b, c, d = v[0:8], v[8:16], v[16:24], v[24:32]
        cos_r, sin_r, cos_c, sin_c = tables
        return jnp.concatenate(
            [a * cos_r - b * sin_r, b * cos_r + a * sin_r, c * cos_c - d * sin_c, d * cos_c + c * sin_c], axis=0
        )

    scale_row = lax.rsqrt(jnp.sum(jnp.transpose(ss[...]), axis=0, keepdims=True) / D + EPS)
    key_rope = turned(aqr[pl.ds(192, ROPE), :] * scale_row).astype(BF16)
    msg[0, 1, pl.ds(T - HALF, ROPE), :] = key_rope[:, :256]
    msg[0, 1, pl.ds(T - HALF + ROPE, ROPE), :] = key_rope[:, 256:]

    s0, s1 = pl.ds(0, SUB), pl.ds(SUB, SUB)

    def key_send(step, sub, to_right):
        d_from, d_to = (step, step + 1) if to_right else ((NZ - step) % NZ, NZ - 1 - step)
        return remote(msg.at[d_from, core, sub], msg.at[d_to, core, sub], zr if to_right else zl)

    zr_a, zl_b = key_send(0, s0, True), key_send(0, s1, False)
    zr_b, zl_a = key_send(0, s1, True), key_send(0, s0, False)

    q_scale = scale_row * ((NOPE + ROPE) ** (-0.5) * math.log2(math.e))
    for h in range(2):
        qs[0, h, pl.ds(0, NOPE), :] = (aqr[pl.ds(96 * h, NOPE), :] * q_scale).astype(BF16)
        qs[0, h, pl.ds(NOPE, ROPE), :] = turned(aqr[pl.ds(96 * h + NOPE, ROPE), :] * q_scale).astype(BF16)
    q96 = pl.ds(0, 96)
    qr0 = remote(qs.at[0, 0, q96], qs.at[1, 0, q96], yr)
    ql0 = remote(qs.at[0, 1, q96], qs.at[2, 1, q96], yl)
    qr1 = remote(qs.at[0, 1, q96], qs.at[1, 1, q96], yr)
    ql1 = remote(qs.at[0, 0, q96], qs.at[2, 0, q96], yl)

    w0, w1 = pl.ds(0, 64), pl.ds(64, 64)
    wr0 = remote(wall.at[0, 0, w0], wall.at[1, 0, w0], xr)
    wl0 = remote(wall.at[0, 0, w1], wall.at[2, 0, w1], xl)
    wr1 = remote(wall.at[0, 0, w1], wall.at[1, 0, w1], xr)
    wl1 = remote(wall.at[0, 0, w0], wall.at[2, 0, w0], xl)
    wd0 = remote(wall.at[0, 0], wall.at[0, 1], partner)

    place = {d: n * T for n, d in enumerate(ARRIVAL)}

    def build(d):
        piece = jnp.concatenate([msg[d, 0], msg[d, 1]], axis=0)
        lat = piece[:T]
        for g in range(2):
            pk = jnp.transpose(piece[T + ROPE * g : T + ROPE * (g + 1)].astype(F32)).astype(BF16)
            k = mm(lat[256 * g : 256 * (g + 1)], ku2[...]) + mm(pk, e_k[...])
            kall[pl.ds(place[d] + 256 * g, 256), :] = k.astype(BF16)
        v = lax.dot_general(vu_t[...], lat, (((1,), (1,)), ((), ())), preferred_element_type=F32).astype(BF16)
        for h in range(2):
            vt[h, pl.ds(0, VDIM), pl.ds(place[d], T)] = v[VDIM * h : VDIM * (h + 1)]

    build(0)

    project(6, right, other, early=False)
    project(3, across, core, early=False)
    project(7, across, other, early=False)
    rounded = lambda k: (a5[:, 128 * k : 128 * (k + 1)] * scale).astype(BF16).astype(F32)
    cprod[...] = (rounded(1) * rounded(0)).astype(BF16)
    to_next = remote(cprod.at[pl.ds(T - 16, 16)], halo.at[0], span_next)
    to_prev = remote(cprod.at[pl.ds(0, 16)], halo.at[1], span_prev)

    right_a, left_b, right_b, left_a, swaps = {0: zr_a}, {0: zl_b}, {0: zr_b}, {0: zl_a}, {}

    def step_a(step):
        right_a[step - 1].wait_recv()
        if step < 4:
            right_a[step] = key_send(step, s0, True)
        left_b[step - 1].wait_recv()
        if step < 4:
            left_b[step] = key_send(step, s1, False)
        else:
            swaps[4] = remote(msg.at[4, core], msg.at[4, core], partner)

    def step_b(step):
        right_b[step - 1].wait_recv()
        if step < 3:
            right_b[step] = key_send(step, s1, True)
        left_a[step - 1].wait_recv()
        if step < 3:
            left_a[step] = key_send(step, s0, False)
        for d in (step, NZ - step):
            swaps[d] = remote(msg.at[d, core], msg.at[d, core], partner)

    def arrive(*pieces):
        for d in pieces:
            swaps[d].wait_recv()
        for d in pieces:
            build(d)

    groups = ((0, 3), (3, 2), (5, 3))

    def stage(new, old, top_old):
        top_new = None
        if new is not None:
            (first, count), i, h = groups[new[0]], new[1], new[2]
            mx = None
            for j in range(count * T // CHUNK):
                s = mm(kall[pl.ds(first * T + j * CHUNK, CHUNK), 128 * h : 128 * (h + 1)], qs[i, h])
                sbuf[h, pl.ds(j * CHUNK, CHUNK), :] = s
                m = jnp.max(s.reshape(CHUNK // 8, 8, T), axis=0)
                mx = m if mx is None else jnp.maximum(mx, m)
            top_new = jnp.max(mx, axis=0, keepdims=True)
        if old is not None:
            (first, count), i, h = groups[old[0]], old[1], old[2]
            if old[0] > 0:
                before = tops[i, h, pl.ds(0, 1), :]
                top_old = jnp.maximum(before, top_old)
            total = None
            for j in range(count * T // CHUNK):
                p = jnp.exp2(sbuf[h, pl.ds(j * CHUNK, CHUNK), :] - top_old).astype(BF16)
                term = mm(vt[h, :, pl.ds(first * T + j * CHUNK, CHUNK)], p)
                total = term if total is None else total + term
            if old[0] > 0:
                total = total + acc[i, h] * jnp.exp2(before - top_old)
            acc[i, h] = total
            tops[i, h] = jnp.broadcast_to(top_old, (8, T))
        return top_new

    def finish(i, h):
        total = acc[i, h, pl.ds(VDIM, 1), :]
        om[i, h] = (acc[i, h, pl.ds(0, VDIM), :] * (1.0 / total)).astype(BF16)
        ostat[i, h] = jnp.concatenate([tops[i, h, pl.ds(0, 1), :], total], axis=0)

    def merged(parts):
        parts = [(o[...].astype(F32), st[...]) for o, st in parts]
        top = parts[0][1][0:1]
        for _, st in parts[1:]:
            top = jnp.maximum(top, st[0:1])
        weights = [st[1:2] * jnp.exp2(st[0:1] - top) for _, st in parts]
        total, summed = weights[0], parts[0][0] * weights[0]
        for w, (o, _) in zip(weights[1:], parts[1:]):
            total, summed = total + w, summed + o * w
        return summed / total, jnp.concatenate([top, total], axis=0)

    lo, hi = slice(0, 1024), slice(1024, 2048)
    order = (2, 1, 3, 0)
    sums = {}

    def conv_rows(c):
        at = lambda r: pl.ds(pl.multiple_of((x + r) % NX * 128 + c * 64, 64), 64)
        return jnp.concatenate([conv_out[at(r), :] for r in range(NX)], axis=0)

    def conv_partials():
        theirs, ours = conv_rows(other), conv_rows(core)
        for n in range(4):
            cols = slice(512 * n, 512 * (n + 1))
            term = mm(theirs, wd[:, cols]).astype(BF16)
            for r in range(NX):
                p_send[r, :, cols] = term[64 * r : 64 * (r + 1)]
        for r in order:
            sums[r] = remote(p_send.at[r], p_recv.at[r], partner)
        for n in range(4):
            cols = slice(512 * n, 512 * (n + 1))
            term = mm(ours, wd[:, cols])
            for r in range(NX):
                own[r, :, cols] = term[64 * r : 64 * (r + 1)]

    def conv_first():
        sums[2].wait_recv()
        for k, cols in enumerate((lo, hi)):
            pair2[k] = (own[2, :, cols] + p_recv[2, :, cols].astype(F32)).astype(BF16)
        sums["a"] = remote(pair2.at[0], turn_a, xr)
        sums["b"] = remote(pair2.at[1], turn_b, xl)
        sums[1].wait_recv()
        pair1[1] = (own[1, :, hi] + p_recv[1, :, hi].astype(F32)).astype(BF16)
        sums["far_r"] = remote(pair1.at[1], from_l.at[1], xr)
        sums[3].wait_recv()
        pair3[0] = (own[3, :, lo] + p_recv[3, :, lo].astype(F32)).astype(BF16)
        sums["far_l"] = remote(pair3.at[0], from_r.at[0], xl)

    def conv_second():
        sums["a"].wait_recv()
        pair1[0] = (own[1, :, lo] + p_recv[1, :, lo].astype(F32) + turn_a[...].astype(F32)).astype(BF16)
        sums["near_r"] = remote(pair1.at[0], from_l.at[0], xr)
        sums["b"].wait_recv()
        pair3[1] = (own[3, :, hi] + p_recv[3, :, hi].astype(F32) + turn_b[...].astype(F32)).astype(BF16)
        sums["near_l"] = remote(pair3.at[1], from_r.at[1], xl)

    weight_hops = {}

    def weights_on(k):
        if k == 0:
            wr0.wait_recv()
            weight_hops["r"] = remote(wall.at[1, 0, w0], wall.at[3, 0, w0], xr)
            wl0.wait_recv()
            weight_hops["l"] = remote(wall.at[2, 0, w1], wall.at[3, 0, w1], xl)
        elif k == 1:
            wr1.wait_recv()
            weight_hops[1] = remote(wall.at[1, 0], wall.at[1, 1], partner)
            wl1.wait_recv()
            weight_hops[2] = remote(wall.at[2, 0], wall.at[2, 1], partner)
        else:
            weight_hops["r"].wait_recv()
            weight_hops["l"].wait_recv()
            weight_hops[3] = remote(wall.at[3, 0], wall.at[3, 1], partner)

    step_a(1)
    step_b(1)
    qr0.wait_recv()
    qr2 = remote(qs.at[1, 0, q96], qs.at[3, 0, q96], yr)
    ql0.wait_recv()
    ql2 = remote(qs.at[2, 1, q96], qs.at[3, 1, q96], yl)
    to_next.wait_recv()
    to_prev.wait_recv()
    cp = cprod[...].astype(F32)
    row = iota((T, 128), 0)
    before = jnp.where(sp > 0, halo[0].astype(F32)[15:16], 0.0)
    after = jnp.where(sp < NY * NZ - 1, halo[1].astype(F32)[0:1], 0.0)
    tap = taps[...].astype(F32)
    mixed = (
        jnp.where(row == 0, before, pltpu.roll(cp, 1, 0)) * tap[0:1]
        + cp * tap[1:2]
        + jnp.where(row == T - 1, after, pltpu.roll(cp, T - 1, 0)) * tap[2:3]
    )
    conv_out[...] = (silu(rounded(3)) * rounded(2) * mixed).astype(BF16)
    gate_out[...] = silu(rounded(4))
    conv_partials()
    arrive(1, 7)

    def key_events(n):
        if n == 0:
            step_a(2)
        elif n == 1:
            weights_on(0)
        elif n == 2:
            qr1.wait_recv()
            ql1.wait_recv()
        elif n == 3:
            step_b(2)
        elif n == 5:
            step_a(3)
            qr2.wait_recv()
            ql2.wait_recv()
        elif n == 7:
            arrive(2, 6)
        elif n == 8:
            step_b(3)
            weights_on(1)
        elif n == 10:
            conv_first()
        elif n == 12:
            step_a(4)
        elif n == 13:
            arrive(3, 5, 4)
        elif n == 16:
            weights_on(2)
        elif n == 19:
            conv_second()

    units = [(0, i, h) for i in (0, 1, 2, 3) for h in range(2)]
    units += [(g, i, h) for g in (1, 2) for i in (3, 2, 1) for h in range(2)]
    units += [(g, 0, h) for g in (1, 2) for h in range(2)]
    back = {}
    top = stage(units[0], None, None)
    for n, (group, i, h) in enumerate(units):
        key_events(n)
        unit = (i, h)
        top = stage(units[n + 1] if n + 1 < len(units) else None, units[n], top)
        if group < 2:
            continue
        finish(i, h)
        if i == 3:
            to = yr if h == 0 else yl
            back[unit] = (remote(om.at[i, h], relay.at[h], to), remote(ostat.at[i, h], relay_stat.at[h], to))
        elif unit == (2, 1):
            back["l", 1] = (remote(om.at[2, 1], ro.at[0, 1], yr), remote(ostat.at[2, 1], rstat.at[0, 1], yr))
        elif unit == (1, 0):
            back["r", 0] = (remote(om.at[1, 0], ro.at[1, 0], yl), remote(ostat.at[1, 0], rstat.at[1, 0], yl))
        elif unit == (1, 1):
            for k, i2, to, side in ((0, 2, yr, "l"), (1, 1, yl, "r")):
                for c in back[(3, k)]:
                    c.wait_recv()
                o, st = merged([(om.at[i2, k], ostat.at[i2, k]), (relay.at[k], relay_stat.at[k])])
                both[k] = o.astype(BF16)
                both_stat[k] = st
                slot = 0 if side == "l" else 1
                back[side, k] = (
                    remote(both.at[k], ro.at[slot, k], to), remote(both_stat.at[k], rstat.at[slot, k], to)
                )
    for side in "lr":
        for k in range(2):
            for c in back[side, k]:
                c.wait_recv()
    parts = [
        merged([(om.at[0, h], ostat.at[0, h])] + [(ro.at[k, h], rstat.at[k, h]) for k in range(2)])[0]
        for h in range(2)
    ]
    attended = jnp.transpose(jnp.concatenate(parts, axis=0))
    aout[...] = (gate_out[...] * attended).astype(BF16)

    def tile(r, c):
        return aout.at[pl.ds(pl.multiple_of((x + r) % NX * 128 + c * 64, 64), 64)]

    tiles = {}
    for r, slot in ((2, 3), (1, 1), (3, 2), (0, 0)):
        for k, c in enumerate((core, other)):
            if r or k:
                tiles[slot, k] = remote(tile(r, c), aall.at[slot, k], tp_peer(r, c) if r else partner)
    aall[0, 0] = tile(0, core)[...]
    for k in (0, "far_r", "far_l", "near_r", "near_l"):
        sums[k].wait_recv()
    for k, cols in enumerate((lo, hi)):
        own[0, :, cols] = (
            own[0, :, cols] + p_recv[0, :, cols].astype(F32) + from_l[k].astype(F32) + from_r[k].astype(F32)
        )
    wd0.wait_recv()
    for k in (1, 2, 3):
        weight_hops[k].wait_recv()
    for slot in range(NX):
        for k in range(2):
            if slot or k:
                tiles[slot, k].wait_recv()
        rows = jnp.concatenate([aall[slot, 0], aall[slot, 1]], axis=1)
        for n in range(4):
            cols = pl.ds(512 * n, 512)
            w = jnp.concatenate([wall[slot, 0, :, cols], wall[slot, 1, :, cols]], axis=0)
            term = own[0, :, cols] + mm(rows, w)
            if slot < NX - 1:
                own[0, :, cols] = term
            else:
                out[:, cols] = term.astype(BF16)
    for c in started:
        c.wait_send()


def scratch():
    v = lambda shape, kind=BF16: pltpu.VMEM(shape, kind)
    return [
        v((8, T, FB)), v((D, 640)), v((224, D)), v((D, 256)),
        v((256, 128)), v((256, 256)), v((256, 128)), v((128, 256)), v((ROPE, 256)), v((128, D)), v((3, 128)), v((256,), F32),
        v((T, 640), F32), v((T, 256), F32), v((224, T), F32), v((T, 128), F32),
        v((NZ, 2, HALF, 256)), v((NY, 2, 128, T)), v((KEYS, 256)), v((2, VROWS, KEYS)),
        v((2, 3 * T, T), F32), v((NY, 2, VROWS, T), F32), v((NY, 2, 8, T), F32),
        v((NY, 2, VDIM, T)), v((NY, 2, 2, T), F32), v((2, 2, VDIM, T)), v((2, 2, 2, T), F32),
        v((2, VDIM, T)), v((2, 2, T), F32), v((2, VDIM, T)), v((2, 2, T), F32),
        v((NX, 2, 128, D)), v((T, 128)), v((NX, 2, 64, 128)),
        v((T, 128)), v((2, 16, 128)), v((T, 128)), v((T, 128), F32),
        v((NX, 64, D)), v((NX, 64, D)), v((NX, 64, D), F32),
        v((2, 64, 1024)), v((2, 64, 1024)), v((2, 64, 1024)), v((64, 1024)), v((64, 1024)),
        v((2, 64, 1024)), v((2, 64, 1024)),
        pltpu.SemaphoreType.DMA((N_REMOTE,)), pltpu.SemaphoreType.DMA((N_REMOTE,)),
        pltpu.SemaphoreType.DMA((N_LOCAL,)),
    ]


def on_device(*args):
    args = tuple(a.T if k in (6, 8) else a for k, a in enumerate(args))
    return pl.pallas_call(
        layer_kernel,
        out_shape=jax.ShapeDtypeStruct((64, D), BF16),
        in_specs=[pl.BlockSpec(memory_space=pl.ANY)] * len(args),
        out_specs=pl.BlockSpec(memory_space=pltpu.VMEM),
        scratch_shapes=scratch(),
        compiler_params=pltpu.CompilerParams(
            collective_id=0, has_side_effects=True, vmem_limit_bytes=62 * 1024 * 1024
        ),
        name="layer",
    )(*args)


def solution(mesh):
    cols, rows, whole = P(None, "tp"), P("tp", None), P()
    placed = (P("sp", "tp"), cols, cols, cols, cols, cols, cols, whole, whole, whole, cols, cols, cols, rows, rows)
    return jax.shard_map(
        on_device, mesh=mesh, in_specs=placed, out_specs=P(("sp", "tp"), None), check_vma=False
    )
```

```python
import math

import jax
import jax.numpy as jnp
from jax import lax
from jax.experimental import pallas as pl
from jax.experimental.pallas import tpu as pltpu
from jax.sharding import PartitionSpec as P

NOPE, ROPE, VDIM, GRID_W = 64, 32, 64, 64
EPS = 1e-06
THETA = 10000.0
D = 2048
T = 512
FB = 256
NX, NY, NZ = 4, 4, 8
KEYS = NZ * T
PIECE = T + 64
HALF = PIECE // 2
SUB = HALF // 2
VROWS = VDIM + 16
CHUNK = 256
ARRIVAL = (0, 1, 7, 2, 6, 3, 5, 4)
N_REMOTE = 96
N_LOCAL = 16
MESH = pl.DeviceIdType.MESH
F32, BF16 = jnp.float32, jnp.bfloat16


def iota(shape, dim):
    return lax.broadcasted_iota(jnp.int32, shape, dim)


def mm(a, b):
    return jnp.dot(a, b, preferred_element_type=F32)


def silu(v):
    return v * (1.0 / (1.0 + jnp.exp(-v)))


def selection(rows, cols, test):
    return jnp.where(test(iota((rows, cols), 0), iota((rows, cols), 1)), 1.0, 0.0).astype(BF16)


def layer_kernel(
    tokens, conv_input, conv_inner, conv_outer, conv_gate, conv_taps, query_proj, latent_proj,
    rope_proj, latent_gain, key_up, value_up, attn_gate, conv_down, attn_down,
    out,
    xall, w5, wqr, wl, ku_raw, ku2, vu_raw, vu_t, e_k, wd, taps, gain,
    a5, al, aqr, ss,
    msg, qs, kall, vt, sbuf, acc, tops,
    om, ostat, ro, rstat, relay, relay_stat, both, both_stat,
    wall, aout, aall, cprod, halo, conv_out, gate_out, p_send, p_recv, own, pair2, pair1, pair3, turn_a, turn_b, from_l, from_r,
    send_sems, recv_sems, local_sems,
):
    sp, tp = lax.axis_index("sp"), lax.axis_index("tp")
    z, y = sp // NY, sp % NY
    x, core = tp // 2, tp % 2
    other = 1 - core
    dev = lambda s, t: {"sp": s, "tp": t}
    partner = dev(sp, x * 2 + other)
    xr, xl = dev(sp, (x + 1) % NX * 2 + core), dev(sp, (x + NX - 1) % NX * 2 + core)
    yr, yl = dev(z * NY + (y + 1) % NY, tp), dev(z * NY + (y + NY - 1) % NY, tp)
    zr, zl = dev((z + 1) % NZ * NY + y, tp), dev((z + NZ - 1) % NZ * NY + y, tp)
    span_next, span_prev = dev((sp + 1) % (NZ * NY), tp), dev((sp + NZ * NY - 1) % (NZ * NY), tp)

    started = []

    def remote(src, dst, to):
        k = len(started)
        copy = pltpu.make_async_remote_copy(
            src_ref=src, dst_ref=dst, send_sem=send_sems.at[k], recv_sem=recv_sems.at[k],
            device_id=to, device_id_type=MESH,
        )
        copy.start()
        started.append(copy)
        return copy

    locals_ = []

    def load(src, dst):
        copy = pltpu.make_async_copy(src, dst, local_sems.at[len(locals_)])
        copy.start()
        locals_.append(copy)
        return copy

    own_block = load(tokens, xall.at[0])
    loads_proj = [load(query_proj, wqr.at[pl.ds(0, 192), :]), load(rope_proj, wqr.at[pl.ds(192, ROPE), :])]
    loads_proj += [
        load(w, w5.at[:, pl.ds(128 * k, 128)])
        for k, w in enumerate((conv_input, conv_inner, conv_outer, conv_gate, attn_gate))
    ]
    loads_proj.append(load(latent_proj, wl))
    loads_late = [load(conv_taps, taps), load(latent_gain, gain)]
    loads_kv = [load(key_up, ku_raw), load(value_up, vu_raw)]
    loads_late += [load(conv_down, wd), load(attn_down, wall.at[0, 0])]

    barrier = pltpu.get_barrier_semaphore()
    tp_peer = lambda r, c: dev(sp, (x + r) % NX * 2 + c)
    peers = [partner, xr, xl, yr, yl, zr, zl, span_next, span_prev]
    for to in peers:
        pl.semaphore_signal(barrier, inc=1, device_id=to, device_id_type=MESH)
    pl.semaphore_wait(barrier, len(peers))

    own_block.wait()
    h0, h1 = pl.ds(0, T // 2), pl.ds(T // 2, T // 2)
    r0 = remote(xall.at[0, h0], xall.at[1, h0], xr)
    l0 = remote(xall.at[0, h1], xall.at[2, h1], xl)
    r1 = remote(xall.at[0, h1], xall.at[1, h1], xr)
    l1 = remote(xall.at[0, h0], xall.at[2, h0], xl)
    d0 = remote(xall.at[0], xall.at[4], partner)

    token = iota((8, T), 1) + sp * T
    entry = iota((8, T), 0)
    freq = jnp.zeros((8, T), F32)
    for j in range(8):
        freq = jnp.where(entry == j, float(THETA ** (-2.0 * j / 16)), freq)
    row_angle = (token // GRID_W).astype(F32) * freq
    col_angle = (token % GRID_W).astype(F32) * freq
    tables = (jnp.cos(row_angle), jnp.sin(row_angle), jnp.cos(col_angle), jnp.sin(col_angle))
    for i in range(NY):
        for h in range(2):
            qs[i, h, pl.ds(96, 32), :] = jnp.zeros((32, T), BF16)
    for h in range(2):
        vt[h, pl.ds(VDIM, 16), :] = jnp.where(iota((16, KEYS), 0) == 0, 1.0, 0.0).astype(BF16)
    for c in loads_proj:
        c.wait()

    def project(slot, chip, c, first=False, early=True, late=True):
        block = pl.multiple_of((chip * 2 + c) * FB, FB)

        def rows_of(i, _):
            rows = pl.ds(pl.multiple_of(i * 256, 256), 256)
            v = xall[slot, rows, :]
            if early:
                wide = v.astype(F32)
                squares = wide[:, :128] * wide[:, :128] + wide[:, 128:] * wide[:, 128:]
                ss[rows, :] = squares if first else ss[rows, :] + squares
                term = lax.dot_general(
                    wqr[:, pl.ds(block, FB)], v, (((1,), (1,)), ((), ())), preferred_element_type=F32
                )
                aqr[:, rows] = term if first else aqr[:, rows] + term
            for total, w, now in ((al, wl, early), (a5, w5, late)):
                if now:
                    term = mm(v, w[pl.ds(block, FB), :])
                    total[rows, :] = term if first else total[rows, :] + term
            return 0

        lax.fori_loop(0, T // 256, rows_of, 0)

    left, right, across = (x + NX - 1) % NX, (x + 1) % NX, (x + 2) % NX
    r0.wait_recv()
    r2 = remote(xall.at[1, h0], xall.at[3, h0], xr)
    l0.wait_recv()
    l2 = remote(xall.at[2, h1], xall.at[3, h1], xl)
    project(0, x, core, first=True)
    d0.wait_recv()
    project(4, x, other)
    for c in loads_kv:
        c.wait()
    ku2[...] = mm(
        ku_raw[...], selection(128, 256, lambda r, c: (c % 128 < 64) & (r == c // 128 * 64 + c % 128))
    ).astype(BF16)
    vu_t[...] = jnp.transpose(vu_raw[...].astype(F32)).astype(BF16)
    e_k[...] = selection(ROPE, 256, lambda r, c: (c % 128 >= 64) & (c % 128 < 96) & (r == c % 128 - 64))
    r1.wait_recv()
    d1 = remote(xall.at[1], xall.at[5], partner)
    l1.wait_recv()
    d2 = remote(xall.at[2], xall.at[6], partner)
    project(1, left, core)
    project(2, right, core)
    d1.wait_recv()
    project(5, left, other)
    r2.wait_recv()
    d3a = remote(xall.at[3, h0], xall.at[7, h0], partner)
    l2.wait_recv()
    d3b = remote(xall.at[3, h1], xall.at[7, h1], partner)
    d2.wait_recv()
    project(6, right, other, late=False)
    project(3, across, core, late=False)
    d3a.wait_recv()
    d3b.wait_recv()
    project(7, across, other, late=False)
    for c in loads_late:
        c.wait()

    scale = lax.rsqrt(jnp.sum(ss[...], axis=1, keepdims=True) / D + EPS)
    zl_ = al[...] * scale
    latent = zl_ * lax.rsqrt(jnp.mean(zl_ * zl_, axis=1, keepdims=True) + EPS) * gain[...].reshape(1, 256)
    latent = latent.astype(BF16)
    msg[0, 0] = latent[:HALF]
    msg[0, 1, pl.ds(0, T - HALF), :] = latent[HALF:]

    def turned(v):
        a, b, c, d = v[0:8], v[8:16], v[16:24], v[24:32]
        cos_r, sin_r, cos_c, sin_c = tables
        return jnp.concatenate(
            [a * cos_r - b * sin_r, b * cos_r + a * sin_r, c * cos_c - d * sin_c, d * cos_c + c * sin_c], axis=0
        )

    scale_row = lax.rsqrt(jnp.sum(jnp.transpose(ss[...]), axis=0, keepdims=True) / D + EPS)
    key_rope = turned(aqr[pl.ds(192, ROPE), :] * scale_row).astype(BF16)
    msg[0, 1, pl.ds(T - HALF, ROPE), :] = key_rope[:, :256]
    msg[0, 1, pl.ds(T - HALF + ROPE, ROPE), :] = key_rope[:, 256:]

    s0, s1 = pl.ds(0, SUB), pl.ds(SUB, SUB)

    def key_send(step, sub, to_right):
        d_from, d_to = (step, step + 1) if to_right else ((NZ - step) % NZ, NZ - 1 - step)
        return remote(msg.at[d_from, core, sub], msg.at[d_to, core, sub], zr if to_right else zl)

    zr_a, zl_b = key_send(0, s0, True), key_send(0, s1, False)
    zr_b, zl_a = key_send(0, s1, True), key_send(0, s0, False)

    q_scale = scale_row * ((NOPE + ROPE) ** (-0.5) * math.log2(math.e))
    for h in range(2):
        qs[0, h, pl.ds(0, NOPE), :] = (aqr[pl.ds(96 * h, NOPE), :] * q_scale).astype(BF16)
        qs[0, h, pl.ds(NOPE, ROPE), :] = turned(aqr[pl.ds(96 * h + NOPE, ROPE), :] * q_scale).astype(BF16)
    q96 = pl.ds(0, 96)
    qr0 = remote(qs.at[0, 0, q96], qs.at[1, 0, q96], yr)
    ql0 = remote(qs.at[0, 1, q96], qs.at[2, 1, q96], yl)
    qr1 = remote(qs.at[0, 1, q96], qs.at[1, 1, q96], yr)
    ql1 = remote(qs.at[0, 0, q96], qs.at[2, 0, q96], yl)

    w0, w1 = pl.ds(0, 64), pl.ds(64, 64)
    wr0 = remote(wall.at[0, 0, w0], wall.at[1, 0, w0], xr)
    wl0 = remote(wall.at[0, 0, w1], wall.at[2, 0, w1], xl)
    wr1 = remote(wall.at[0, 0, w1], wall.at[1, 0, w1], xr)
    wl1 = remote(wall.at[0, 0, w0], wall.at[2, 0, w0], xl)
    wd0 = remote(wall.at[0, 0], wall.at[0, 1], partner)

    place = {d: n * T for n, d in enumerate(ARRIVAL)}

    def build(d):
        piece = jnp.concatenate([msg[d, 0], msg[d, 1]], axis=0)
        lat = piece[:T]
        for g in range(2):
            pk = jnp.transpose(piece[T + ROPE * g : T + ROPE * (g + 1)].astype(F32)).astype(BF16)
            k = mm(lat[256 * g : 256 * (g + 1)], ku2[...]) + mm(pk, e_k[...])
            kall[pl.ds(place[d] + 256 * g, 256), :] = k.astype(BF16)
        v = lax.dot_general(vu_t[...], lat, (((1,), (1,)), ((), ())), preferred_element_type=F32).astype(BF16)
        for h in range(2):
            vt[h, pl.ds(0, VDIM), pl.ds(place[d], T)] = v[VDIM * h : VDIM * (h + 1)]

    build(0)

    project(6, right, other, early=False)
    project(3, across, core, early=False)
    project(7, across, other, early=False)
    rounded = lambda k: (a5[:, 128 * k : 128 * (k + 1)] * scale).astype(BF16).astype(F32)
    cprod[...] = (rounded(1) * rounded(0)).astype(BF16)
    to_next = remote(cprod.at[pl.ds(T - 16, 16)], halo.at[0], span_next)
    to_prev = remote(cprod.at[pl.ds(0, 16)], halo.at[1], span_prev)

    right_a, left_b, right_b, left_a, swaps = {0: zr_a}, {0: zl_b}, {0: zr_b}, {0: zl_a}, {}

    def step_a(step):
        right_a[step - 1].wait_recv()
        if step < 4:
            right_a[step] = key_send(step, s0, True)
        left_b[step - 1].wait_recv()
        if step < 4:
            left_b[step] = key_send(step, s1, False)
        else:
            swaps[4] = remote(msg.at[4, core], msg.at[4, core], partner)

    def step_b(step):
        right_b[step - 1].wait_recv()
        if step < 3:
            right_b[step] = key_send(step, s1, True)
        left_a[step - 1].wait_recv()
        if step < 3:
            left_a[step] = key_send(step, s0, False)
        for d in (step, NZ - step):
            swaps[d] = remote(msg.at[d, core], msg.at[d, core], partner)

    def arrive(*pieces):
        for d in pieces:
            swaps[d].wait_recv()
        for d in pieces:
            build(d)

    groups = ((0, 3), (3, 2), (5, 3))

    def stage(new, old, top_old):
        top_new = None
        if new is not None:
            (first, count), i, h = groups[new[0]], new[1], new[2]
            mx = None
            for j in range(count * T // CHUNK):
                s = mm(kall[pl.ds(first * T + j * CHUNK, CHUNK), 128 * h : 128 * (h + 1)], qs[i, h])
                sbuf[h, pl.ds(j * CHUNK, CHUNK), :] = s
                m = jnp.max(s.reshape(CHUNK // 8, 8, T), axis=0)
                mx = m if mx is None else jnp.maximum(mx, m)
            top_new = jnp.max(mx, axis=0, keepdims=True)
        if old is not None:
            (first, count), i, h = groups[old[0]], old[1], old[2]
            if old[0] > 0:
                before = tops[i, h, pl.ds(0, 1), :]
                top_old = jnp.maximum(before, top_old)
            total = None
            for j in range(count * T // CHUNK):
                p = jnp.exp2(sbuf[h, pl.ds(j * CHUNK, CHUNK), :] - top_old).astype(BF16)
                term = mm(vt[h, :, pl.ds(first * T + j * CHUNK, CHUNK)], p)
                total = term if total is None else total + term
            if old[0] > 0:
                total = total + acc[i, h] * jnp.exp2(before - top_old)
            acc[i, h] = total
            tops[i, h] = jnp.broadcast_to(top_old, (8, T))
        return top_new

    def finish(i, h):
        total = acc[i, h, pl.ds(VDIM, 1), :]
        om[i, h] = (acc[i, h, pl.ds(0, VDIM), :] * (1.0 / total)).astype(BF16)
        ostat[i, h] = jnp.concatenate([tops[i, h, pl.ds(0, 1), :], total], axis=0)

    def merged(parts):
        parts = [(o[...].astype(F32), st[...]) for o, st in parts]
        top = parts[0][1][0:1]
        for _, st in parts[1:]:
            top = jnp.maximum(top, st[0:1])
        weights = [st[1:2] * jnp.exp2(st[0:1] - top) for _, st in parts]
        total, summed = weights[0], parts[0][0] * weights[0]
        for w, (o, _) in zip(weights[1:], parts[1:]):
            total, summed = total + w, summed + o * w
        return summed / total, jnp.concatenate([top, total], axis=0)

    lo, hi = slice(0, 1024), slice(1024, 2048)
    order = (2, 1, 3, 0)
    sums = {}

    def conv_rows(c):
        at = lambda r: pl.ds(pl.multiple_of((x + r) % NX * 128 + c * 64, 64), 64)
        return jnp.concatenate([conv_out[at(r), :] for r in range(NX)], axis=0)

    def conv_partials():
        theirs, ours = conv_rows(other), conv_rows(core)
        for n in range(4):
            cols = slice(512 * n, 512 * (n + 1))
            term = mm(theirs, wd[:, cols]).astype(BF16)
            for r in range(NX):
                p_send[r, :, cols] = term[64 * r : 64 * (r + 1)]
        for r in order:
            sums[r] = remote(p_send.at[r], p_recv.at[r], partner)
        for n in range(4):
            cols = slice(512 * n, 512 * (n + 1))
            term = mm(ours, wd[:, cols])
            for r in range(NX):
                own[r, :, cols] = term[64 * r : 64 * (r + 1)]

    def conv_first():
        sums[2].wait_recv()
        for k, cols in enumerate((lo, hi)):
            pair2[k] = (own[2, :, cols] + p_recv[2, :, cols].astype(F32)).astype(BF16)
        sums["a"] = remote(pair2.at[0], turn_a, xr)
        sums["b"] = remote(pair2.at[1], turn_b, xl)
        sums[1].wait_recv()
        pair1[1] = (own[1, :, hi] + p_recv[1, :, hi].astype(F32)).astype(BF16)
        sums["far_r"] = remote(pair1.at[1], from_l.at[1], xr)
        sums[3].wait_recv()
        pair3[0] = (own[3, :, lo] + p_recv[3, :, lo].astype(F32)).astype(BF16)
        sums["far_l"] = remote(pair3.at[0], from_r.at[0], xl)

    def conv_second():
        sums["a"].wait_recv()
        pair1[0] = (own[1, :, lo] + p_recv[1, :, lo].astype(F32) + turn_a[...].astype(F32)).astype(BF16)
        sums["near_r"] = remote(pair1.at[0], from_l.at[0], xr)
        sums["b"].wait_recv()
        pair3[1] = (own[3, :, hi] + p_recv[3, :, hi].astype(F32) + turn_b[...].astype(F32)).astype(BF16)
        sums["near_l"] = remote(pair3.at[1], from_r.at[1], xl)

    weight_hops = {}

    def weights_on(k):
        if k == 0:
            wr0.wait_recv()
            weight_hops["r"] = remote(wall.at[1, 0, w0], wall.at[3, 0, w0], xr)
            wl0.wait_recv()
            weight_hops["l"] = remote(wall.at[2, 0, w1], wall.at[3, 0, w1], xl)
        elif k == 1:
            wr1.wait_recv()
            weight_hops[1] = remote(wall.at[1, 0], wall.at[1, 1], partner)
            wl1.wait_recv()
            weight_hops[2] = remote(wall.at[2, 0], wall.at[2, 1], partner)
        else:
            weight_hops["r"].wait_recv()
            weight_hops["l"].wait_recv()
            weight_hops[3] = remote(wall.at[3, 0], wall.at[3, 1], partner)

    step_a(1)
    step_b(1)
    qr0.wait_recv()
    qr2 = remote(qs.at[1, 0, q96], qs.at[3, 0, q96], yr)
    ql0.wait_recv()
    ql2 = remote(qs.at[2, 1, q96], qs.at[3, 1, q96], yl)
    to_next.wait_recv()
    to_prev.wait_recv()
    cp = cprod[...].astype(F32)
    row = iota((T, 128), 0)
    before = jnp.where(sp > 0, halo[0].astype(F32)[15:16], 0.0)
    after = jnp.where(sp < NY * NZ - 1, halo[1].astype(F32)[0:1], 0.0)
    tap = taps[...].astype(F32)
    mixed = (
        jnp.where(row == 0, before, pltpu.roll(cp, 1, 0)) * tap[0:1]
        + cp * tap[1:2]
        + jnp.where(row == T - 1, after, pltpu.roll(cp, T - 1, 0)) * tap[2:3]
    )
    conv_out[...] = (silu(rounded(3)) * rounded(2) * mixed).astype(BF16)
    gate_out[...] = silu(rounded(4))
    conv_partials()
    arrive(1, 7)

    def key_events(n):
        if n == 0:
            step_a(2)
        elif n == 1:
            weights_on(0)
        elif n == 2:
            qr1.wait_recv()
            ql1.wait_recv()
        elif n == 3:
            step_b(2)
        elif n == 5:
            step_a(3)
            qr2.wait_recv()
            ql2.wait_recv()
        elif n == 7:
            arrive(2, 6)
        elif n == 8:
            step_b(3)
            weights_on(1)
        elif n == 10:
            conv_first()
        elif n == 12:
            step_a(4)
        elif n == 13:
            arrive(3, 5, 4)
        elif n == 16:
            weights_on(2)
        elif n == 19:
            conv_second()

    units = [(0, i, h) for i in (0, 1, 2, 3) for h in range(2)]
    units += [(g, i, h) for g in (1, 2) for i in (3, 2, 1) for h in range(2)]
    units += [(g, 0, h) for g in (1, 2) for h in range(2)]
    back = {}
    top = stage(units[0], None, None)
    for n, (group, i, h) in enumerate(units):
        key_events(n)
        unit = (i, h)
        top = stage(units[n + 1] if n + 1 < len(units) else None, units[n], top)
        if group < 2:
            continue
        finish(i, h)
        if i == 3:
            to = yr if h == 0 else yl
            back[unit] = (remote(om.at[i, h], relay.at[h], to), remote(ostat.at[i, h], relay_stat.at[h], to))
        elif unit == (2, 1):
            back["l", 1] = (remote(om.at[2, 1], ro.at[0, 1], yr), remote(ostat.at[2, 1], rstat.at[0, 1], yr))
        elif unit == (1, 0):
            back["r", 0] = (remote(om.at[1, 0], ro.at[1, 0], yl), remote(ostat.at[1, 0], rstat.at[1, 0], yl))
        elif unit == (1, 1):
            for k, i2, to, side in ((0, 2, yr, "l"), (1, 1, yl, "r")):
                for c in back[(3, k)]:
                    c.wait_recv()
                o, st = merged([(om.at[i2, k], ostat.at[i2, k]), (relay.at[k], relay_stat.at[k])])
                both[k] = o.astype(BF16)
                both_stat[k] = st
                slot = 0 if side == "l" else 1
                back[side, k] = (
                    remote(both.at[k], ro.at[slot, k], to), remote(both_stat.at[k], rstat.at[slot, k], to)
                )
    for side in "lr":
        for k in range(2):
            for c in back[side, k]:
                c.wait_recv()
    parts = [
        merged([(om.at[0, h], ostat.at[0, h])] + [(ro.at[k, h], rstat.at[k, h]) for k in range(2)])[0]
        for h in range(2)
    ]
    attended = jnp.transpose(jnp.concatenate(parts, axis=0))
    aout[...] = (gate_out[...] * attended).astype(BF16)

    def tile(r, c):
        return aout.at[pl.ds(pl.multiple_of((x + r) % NX * 128 + c * 64, 64), 64)]

    tiles = {}
    for r, slot in ((2, 3), (1, 1), (3, 2), (0, 0)):
        for k, c in enumerate((core, other)):
            if r or k:
                tiles[slot, k] = remote(tile(r, c), aall.at[slot, k], tp_peer(r, c) if r else partner)
    aall[0, 0] = tile(0, core)[...]
    for k in (0, "far_r", "far_l", "near_r", "near_l"):
        sums[k].wait_recv()
    for k, cols in enumerate((lo, hi)):
        own[0, :, cols] = (
            own[0, :, cols] + p_recv[0, :, cols].astype(F32) + from_l[k].astype(F32) + from_r[k].astype(F32)
        )
    wd0.wait_recv()
    for k in (1, 2, 3):
        weight_hops[k].wait_recv()
    for slot in range(NX):
        for k in range(2):
            if slot or k:
                tiles[slot, k].wait_recv()
        rows = jnp.concatenate([aall[slot, 0], aall[slot, 1]], axis=1)
        for n in range(4):
            cols = pl.ds(512 * n, 512)
            w = jnp.concatenate([wall[slot, 0, :, cols], wall[slot, 1, :, cols]], axis=0)
            term = own[0, :, cols] + mm(rows, w)
            if slot < NX - 1:
                own[0, :, cols] = term
            else:
                out[:, cols] = term.astype(BF16)
    for c in started:
        c.wait_send()


def scratch():
    v = lambda shape, kind=BF16: pltpu.VMEM(shape, kind)
    return [
        v((8, T, FB)), v((D, 640)), v((224, D)), v((D, 256)),
        v((256, 128)), v((256, 256)), v((256, 128)), v((128, 256)), v((ROPE, 256)), v((128, D)), v((3, 128)), v((256,), F32),
        v((T, 640), F32), v((T, 256), F32), v((224, T), F32), v((T, 128), F32),
        v((NZ, 2, HALF, 256)), v((NY, 2, 128, T)), v((KEYS, 256)), v((2, VROWS, KEYS)),
        v((2, 3 * T, T), F32), v((NY, 2, VROWS, T), F32), v((NY, 2, 8, T), F32),
        v((NY, 2, VDIM, T)), v((NY, 2, 2, T), F32), v((2, 2, VDIM, T)), v((2, 2, 2, T), F32),
        v((2, VDIM, T)), v((2, 2, T), F32), v((2, VDIM, T)), v((2, 2, T), F32),
        v((NX, 2, 128, D)), v((T, 128)), v((NX, 2, 64, 128)),
        v((T, 128)), v((2, 16, 128)), v((T, 128)), v((T, 128), F32),
        v((NX, 64, D)), v((NX, 64, D)), v((NX, 64, D), F32),
        v((2, 64, 1024)), v((2, 64, 1024)), v((2, 64, 1024)), v((64, 1024)), v((64, 1024)),
        v((2, 64, 1024)), v((2, 64, 1024)),
        pltpu.SemaphoreType.DMA((N_REMOTE,)), pltpu.SemaphoreType.DMA((N_REMOTE,)),
        pltpu.SemaphoreType.DMA((N_LOCAL,)),
    ]


def on_device(*args):
    args = tuple(a.T if k in (6, 8) else a for k, a in enumerate(args))
    return pl.pallas_call(
        layer_kernel,
        out_shape=jax.ShapeDtypeStruct((64, D), BF16),
        in_specs=[pl.BlockSpec(memory_space=pl.ANY)] * len(args),
        out_specs=pl.BlockSpec(memory_space=pltpu.VMEM),
        scratch_shapes=scratch(),
        compiler_params=pltpu.CompilerParams(
            collective_id=0, has_side_effects=True, vmem_limit_bytes=62 * 1024 * 1024
        ),
        name="layer",
    )(*args)


def solution(mesh):
    cols, rows, whole = P(None, "tp"), P("tp", None), P()
    placed = (P("sp", "tp"), cols, cols, cols, cols, cols, cols, whole, whole, whole, cols, cols, cols, rows, rows)
    return jax.shard_map(
        on_device, mesh=mesh, in_specs=placed, out_specs=P(("sp", "tp"), None), check_vma=False
    )
```
